256 devices in a mesh: grp: 2 (over y), sp: 32 (over z, core), tp: 4 (over x).
Axes of the slice: x: 4, y: 2, z: 16, core: 2. Of those that a mesh axis runs over, the one named last changes fastest.
The devices are a block of a 4x16x16 slice.
Arguments:
- residual_in: bfloat16 [8192, 2048], P(('grp', 'sp'), 'tp'), parts along dimension 0, may hold values from -16 to 16
- query_pre: bfloat16 [8192, 512], P(('grp', 'sp'), 'tp'), parts along dimension 0, may hold values from -6 to 6
- forget_pre: bfloat16 [8192, 512], P(('grp', 'sp'), 'tp'), parts along dimension 0, may hold values from -9 to 9
- value_pre: bfloat16 [8192, 512], P(('grp', 'sp'), 'tp'), parts along dimension 0, may hold values from -6 to 6
- gate_pre: bfloat16 [8192, 512], P(('grp', 'sp'), 'tp'), parts along dimension 0, may hold values from -6 to 6
- floor_gap: float32 [512], P('tp'), may hold values from 0 to 1, as said below
- head_gain: float32 [64], replicated, may hold values from 0.1 to 1.9
- out_weight: bfloat16 [512, 2048], P(None, 'tp'), may hold values from -0.25 to 0.25
- norm_gain: float32 [2048], P('tp'), may hold values from 0.1 to 1.9
- value_weight: bfloat16 [2048, 5632], P('sp', 'tp'), may hold values from -0.125 to 0.125
- gate_weight: bfloat16 [2048, 5632], P('sp', 'tp'), may hold values from -0.125 to 0.125
- value_taps: float32 [3, 5632], P(None, 'tp'), may hold values from -3 to 3
- gate_taps: float32 [3, 5632], P(None, 'tp'), may hold values from -3 to 3
- down_weight: bfloat16 [5632, 2048], P('tp', 'sp'), may hold values from -0.078125 to 0.078125
Outputs:
- mixed: bfloat16 [8192, 2048], P(('grp', 'sp'), 'tp'), parts along dimension 0
The draws below stay inside these ranges and needn't reach their ends.
There are 2 independent parts, one for each index of `grp`. The reference program is written for one: setup_inputs(seed, part) draws one part's arguments, and reference() takes and returns one part's arrays. A program takes and returns all parts, laid end to end along the dimension named above; an argument that names none is the same for every part. Nothing has to cross between parts.
Inputs may be any that keep to these rules, and one draw needn't show every extreme that they name: `floor_gap`: each channel's value lies strictly between 0 and 1.
All inputs are finite; a program needn't handle non-finite values.
Results may differ from the reference program's by a relative error of at most 0.0085.
Values may be sent and summed in bfloat16 or wider, within the bound.
No kernel may reach another device: no remote copies, remote signals or barrier semaphores. Data moves between devices by JAX's collectives and lax.ppermute only.
A program may use at most 128 MiB of HBM per device.

```python
import jax
import jax.numpy as jnp
from jax import lax

D = 2048
H = 8
DK = 64
DV = 64
FF = 5632
TAPS = 3
BLOCK = 64
TOK_DEV = 128
TOKENS = 4096


def draw_residual_in(key, part):
    noise_key, order_key = jax.random.split(jax.random.fold_in(key, 11))
    base = jax.random.normal(noise_key, (TOKENS, D), jnp.float32)
    ranking = jax.random.permutation(order_key, 4).astype(jnp.float32)
    scales = 0.35 * 6.0 ** (ranking / 3.0)
    return (base.reshape(TOKENS, 4, D // 4) * scales[None, :, None]).reshape(TOKENS, D).astype(jnp.bfloat16)


def draw_forget_pre(key, part):
    noise_key, offset_key = jax.random.split(jax.random.fold_in(key, 17))
    base = jnp.clip(jax.random.normal(noise_key, (TOKENS, H * DK), jnp.float32), -6.0, 6.0)
    offsets = jax.random.uniform(offset_key, (TOKENS // TOK_DEV, 1, H * DK), jnp.float32, -1.5, 1.5)
    return (base.reshape(TOKENS // TOK_DEV, TOK_DEV, H * DK) + offsets).reshape(TOKENS, H * DK).astype(jnp.bfloat16)


def draw_floor_gap(key, part):
    order_key, slow_key, fast_key = jax.random.split(jax.random.fold_in(key, 23), 3)
    ranking = jax.random.permutation(order_key, H)
    quick = ranking < H // 2
    slow_values = jnp.exp(jax.random.uniform(slow_key, (H, DK), jnp.float32, jnp.log(0.3 / TOKENS), jnp.log(2.5 / TOKENS)))
    fast_values = jnp.exp(jax.random.uniform(fast_key, (H, DK), jnp.float32, jnp.log(0.02), jnp.log(0.06)))
    return jnp.where(quick[:, None], fast_values, slow_values).reshape(H * DK)


def shard_levels(rng, dims, cuts, least, largest):
    gain, own = 1.0, jax.random.fold_in(rng, 6)
    for dim, blocks in cuts:
        heights = jnp.exp(jax.random.uniform(jax.random.fold_in(own, dim), (blocks,), jnp.float32, least / len(cuts), largest / len(cuts)))
        gain = gain * jnp.repeat(heights, dims[dim] // blocks).reshape([-1 if axis == dim else 1 for axis in range(len(dims))])
    return gain


def centred(rng, extent, scale, reach, shards=(), kind=jnp.bfloat16):
    factor_of = shard_levels(rng, extent, shards, -0.22, 0.18) if shards else 1.0
    values = jax.random.normal(rng, extent, jnp.float32) * scale * factor_of
    return jnp.minimum(jnp.maximum(values, -reach), reach).astype(kind)


def setup_inputs(seed: int = 0, part: int = 0) -> dict:
    streams_of = jax.random.split(jax.random.key(seed), 15)
    part_keys = jax.random.split(jax.random.fold_in(streams_of[14], part), 15)
    return {
        "residual_in": draw_residual_in(jax.random.fold_in(jax.random.fold_in(streams_of[14], part), 71), part),
        "query_pre": centred(part_keys[1], (TOKENS, H * DK), 1.0, 6.0, ((0, 32), (1, 4))),
        "forget_pre": draw_forget_pre(jax.random.fold_in(jax.random.fold_in(streams_of[14], part), 71), part),
        "value_pre": centred(part_keys[3], (TOKENS, H * DV), 1.0, 6.0, ((0, 32), (1, 4))),
        "gate_pre": centred(part_keys[4], (TOKENS, H * DV), 1.0, 6.0, ((0, 32), (1, 4))),
        "floor_gap": draw_floor_gap(jax.random.fold_in(streams_of[14], 71), part),
        "head_gain": jnp.clip(1.0 + 0.18 * jax.random.normal(streams_of[6], (DV,), jnp.float32), 0.1, 1.9),
        "out_weight": centred(streams_of[7], (H * DV, D), (H * DV) ** -0.5, 0.25, ((1, 4),)),
        "norm_gain": jnp.clip(1.0 + 0.18 * jax.random.normal(streams_of[8], (D,), jnp.float32), 0.1, 1.9),
        "value_weight": centred(streams_of[9], (D, FF), D ** -0.5, 0.125, ((0, 32), (1, 4))),
        "gate_weight": centred(streams_of[10], (D, FF), D ** -0.5, 0.125, ((0, 32), (1, 4))),
        "value_taps": centred(streams_of[11], (TAPS, FF), 0.577, 3.0, ((1, 4),), jnp.float32),
        "gate_taps": centred(streams_of[12], (TAPS, FF), 0.577, 3.0, ((1, 4),), jnp.float32),
        "down_weight": centred(streams_of[13], (FF, D), FF ** -0.5, 0.078125, ((0, 4), (1, 32))),
    }


epsilon = 1e-06
highest_precision = lax.Precision.HIGHEST

def split_heads(matrix, head_count):
    return matrix.reshape(matrix.shape[0], head_count, -1).transpose(1, 0, 2)

def recurrence(query_rows, gate_keys, values, log_decay, block_size, start_state):
    head_count, seq_length, key_width = query_rows.shape
    block_count = seq_length // block_size

    def to_blocks(tensor):
        return tensor.reshape(head_count, block_count, block_size, tensor.shape[-1]).transpose(1, 0, 2, 3)
    causal = jnp.tril(jnp.ones((block_size, block_size), dtype=bool))

    def advance(current_state, inputs):
        block_queries, block_keys, block_values, decay_block = inputs
        running_state = jnp.cumsum(decay_block, axis=1)
        carried_state = jnp.einsum('pen,pnd->ped', block_queries * jnp.exp(running_state), current_state, precision=highest_precision)
        spread = jnp.where(causal[None, :, :, None], running_state[:, :, None, :] - running_state[:, None, :, :], -jnp.inf)
        scores = jnp.einsum('htk,hsk,htsk->hts', block_queries, block_keys, jnp.exp(spread), precision=highest_precision)
        inner = jnp.einsum('hts,hsv->htv', scores, block_values, precision=highest_precision)
        ending_state = running_state[:, -1, :]
        fresh_update = jnp.einsum('bia,big->bag', block_keys * jnp.exp(ending_state[:, None, :] - running_state), block_values, precision=highest_precision)
        return (jnp.exp(ending_state)[:, :, None] * current_state + fresh_update, carried_state + inner)
    final_state, outputs = lax.scan(advance, start_state, (to_blocks(query_rows), to_blocks(gate_keys), to_blocks(values), to_blocks(log_decay)))
    return (final_state, outputs.transpose(1, 0, 2, 3).reshape(head_count, seq_length, values.shape[-1]))

def mixer_inputs(query_pre, forget_pre, value_pre, floor_gap, head_count):
    gate_keys = floor_gap.astype(jnp.float32) * jax.nn.sigmoid(-forget_pre.astype(jnp.float32))
    log_decay = jnp.log1p(-gate_keys)
    query_rows = jax.nn.silu(query_pre.astype(jnp.float32))
    return (split_heads(query_rows, head_count), split_heads(gate_keys, head_count), split_heads(value_pre.astype(jnp.float32), head_count), split_heads(log_decay, head_count))

def head_output(recurrent, head_gain, gate_pre):
    ordered = recurrent.transpose(1, 0, 2)
    scaled = ordered * lax.rsqrt(lax.optimization_barrier(jnp.mean(ordered * ordered, axis=-1, keepdims=True)) + epsilon) * head_gain
    gating = jax.nn.silu(gate_pre.astype(jnp.float32)).reshape(ordered.shape)
    return (scaled * gating).reshape(ordered.shape[0], -1).astype(jnp.bfloat16)

def causal_taps(padded, taps, row_count):
    return taps[0] * padded[0:row_count] + taps[1] * padded[1:row_count + 1] + taps[2] * padded[2:row_count + 2]

def reference(residual_in, query_pre, forget_pre, value_pre, gate_pre, floor_gap, head_gain, out_weight, norm_gain, value_weight, gate_weight, value_taps, gate_taps, down_weight):
    row_count = residual_in.shape[0]
    query_rows, gate_keys, values, log_decay = mixer_inputs(query_pre, forget_pre, value_pre, floor_gap, H)
    start_state = jnp.zeros((H, DK, DV), jnp.float32)
    final_state, recurrent = recurrence(query_rows, gate_keys, values, log_decay, BLOCK, start_state)
    head_out = head_output(recurrent, head_gain, gate_pre)
    stream = residual_in.astype(jnp.float32) + jnp.dot(head_out, out_weight, preferred_element_type=jnp.float32)
    normed = (stream * lax.rsqrt(lax.optimization_barrier(jnp.mean(stream * stream, axis=1, keepdims=True)) + epsilon) * norm_gain).astype(jnp.bfloat16)
    up_value = jnp.dot(normed, value_weight, preferred_element_type=jnp.float32).astype(jnp.bfloat16)
    up_gate = jnp.dot(normed, gate_weight, preferred_element_type=jnp.float32).astype(jnp.bfloat16)
    zero_rows = jnp.zeros((2, up_value.shape[1]), jnp.float32)
    conv_value = causal_taps(jnp.concatenate([zero_rows, up_value.astype(jnp.float32)], axis=0), value_taps, row_count)
    conv_gate = causal_taps(jnp.concatenate([zero_rows, up_gate.astype(jnp.float32)], axis=0), gate_taps, row_count)
    hidden = (jax.nn.silu(conv_gate) * conv_value).astype(jnp.bfloat16)
    return (stream + jnp.dot(hidden, down_weight, preferred_element_type=jnp.float32)).astype(jnp.bfloat16)
```

```python
import jax
import jax.numpy as jnp
from jax import lax
from jax.experimental import pallas as pl
from jax.experimental.pallas import tpu as pltpu
from jax.sharding import Mesh
from jax.sharding import PartitionSpec as P

BF = jnp.bfloat16
F32 = jnp.float32
EPS = 1e-06
DK = 64
SP = ("sp_0", "sp_1")
GRP = ("grp_0", "grp_1")
PAIR = ("grp_1", "tp")
HALO = 16
CH = 16


def silu(v):
    return v / (1.0 + jnp.exp(-v))


def nt_dot(a, b):
    return lax.dot_general(a, b, (((1,), (1,)), ((), ())), preferred_element_type=F32)


def tn_dot(a, b):
    return lax.dot_general(a, b, (((0,), (0,)), ((), ())), preferred_element_type=F32)


def dot(a, b):
    return jnp.dot(a, b, preferred_element_type=F32)


def iota(shape, dim):
    return lax.broadcasted_iota(jnp.int32, shape, dim)


def in_order(rows, halo):
    count = rows.shape[0]
    both = jnp.concatenate([rows.astype(F32), halo.astype(F32)], axis=0)
    row = iota(both.shape, 0)
    both = jnp.where((row >= count) & (row < count + HALO - 2), 0.0, both)
    return pltpu.roll(both, 2, 0)


def head_ones(width):
    a = iota((width, width), 0) // DK
    b = iota((width, width), 1) // DK
    return jnp.where(a == b, 1.0, 0.0).astype(BF)


def local_kernel(q_ref, f_ref, v_ref, halo_ref, gap_ref, intra_ref, qd_ref, state_ref):
    count, width = q_ref.shape
    q = silu(in_order(q_ref[...], halo_ref[:, 0:width]))
    f = in_order(f_ref[...], halo_ref[:, width : 2 * width])
    v = in_order(v_ref[...], halo_ref[:, 2 * width : 3 * width])
    rows = q.shape[0]
    k = gap_ref[...] / (1.0 + jnp.exp(f))
    a = 1.0 - k
    la = jnp.log(a)
    row = iota(q.shape, 0)
    lane = iota((CH, width), 1)
    r = la
    step = 1
    while step < rows:
        r = r + jnp.where(row >= step, pltpu.roll(r, step, 0), 0.0)
        step *= 2
    ones = head_ones(width)
    inside = row % CH
    decay = jnp.ones_like(q)
    out = jnp.zeros_like(q)
    for j in range(CH):
        if j:
            decay = decay * (pltpu.roll(a, j - 1, 0) if j > 1 else a)
        kj = pltpu.roll(k, j, 0) if j else k
        vj = pltpu.roll(v, j, 0) if j else v
        term = jnp.where(inside >= j, q * decay * kj, 0.0)
        out = out + dot(term.astype(BF), ones) * vj
    pieces = [out[:CH]]
    vb = v.astype(BF)
    for i in range(1, rows // CH):
        lo = i * CH
        start = r[lo - 1 : lo]
        qi = q[lo : lo + CH] * jnp.exp(r[lo : lo + CH] - start)
        qi = jnp.concatenate([jnp.where(lane < DK, qi, 0.0), jnp.where(lane >= DK, qi, 0.0)], axis=0)
        ki = k[:lo] * jnp.exp(start - r[:lo])
        both = dot(nt_dot(qi.astype(BF), ki.astype(BF)).astype(BF), vb[:lo])
        pieces.append(out[lo : lo + CH] + jnp.where(lane < DK, both[:CH], both[CH:]))
    intra_ref[...] = jnp.concatenate(pieces, axis=0)
    qd_ref[...] = (q * jnp.exp(r)).astype(BF)
    last = r[count - 1 : count]
    kf = (k[:count] * jnp.exp(last - r[:count])).astype(BF)
    full = tn_dot(vb[:count], kf)
    half = iota((DK, width), 1)
    state_ref[:DK] = jnp.where(half < DK, full[:DK], full[DK:]).astype(BF)
    state_ref[DK:] = jnp.broadcast_to(jnp.exp(last), (HALO, width)).astype(BF)


def head_kernel(intra_ref, qd_ref, enter_ref, g_ref, halo_ref, gain_ref, out_ref):
    width = intra_ref.shape[1]
    half = iota((DK, width), 1)
    e = enter_ref[...]
    full = jnp.concatenate([jnp.where(half < DK, e, 0.0), jnp.where(half >= DK, e, 0.0)], axis=0)
    rec = intra_ref[...] + nt_dot(qd_ref[...], full.astype(BF))
    ones = head_ones(width)
    sq = rec * rec
    hi = sq.astype(BF)
    lo = (sq - hi.astype(F32)).astype(BF)
    mean = (dot(hi, ones) + dot(lo, ones)) * (1.0 / DK)
    gate = in_order(g_ref[...], halo_ref[...])
    out = rec * lax.rsqrt(mean + EPS) * gain_ref[...] * silu(gate)
    out_ref[...] = pltpu.roll(out, out.shape[0] - 2, 0).astype(BF)


def stream_kernel(x_ref, *refs):
    n = (len(refs) - 2) // 4
    heads, weights, resid, gains = (refs[i * n : (i + 1) * n] for i in range(4))
    normed_ref, own_ref = refs[4 * n :]
    x = x_ref[0]
    hw = heads[0].shape[1]
    cw = resid[0].shape[1]
    head = jnp.concatenate([h[...] for h in heads], axis=1)
    parts = []
    total = None
    for d in range(n):
        w = jnp.concatenate([weights[d][pl.ds(hw * lax.rem(x + e, n), hw), :] for e in range(n)], axis=0)
        s = resid[d][...].astype(F32) + dot(head, w)
        parts.append(s)
        sq = jnp.sum(s * s, axis=1, keepdims=True)
        total = sq if total is None else total + sq
    own_ref[...] = parts[0][: own_ref.shape[0]]
    scale = lax.rsqrt(total / (n * cw) + EPS)
    for d in range(n):
        g = gains[d][...].astype(F32)
        gain = g[0:1] + g[1:2] + g[2:3]
        normed_ref[:, d * cw : (d + 1) * cw] = (parts[d] * scale * gain).astype(BF)


def mixer_kernel(x_ref, normed_ref, taps_ref, w_hbm, out_ref, w, acc, sems):
    n = out_ref.shape[0]
    groups = out_ref.shape[1]
    count = out_ref.shape[2]
    x = x_ref[0]
    cw = w.shape[0] // n
    up = taps_ref.shape[1]
    half = up // 2
    rows = acc.shape[0] // groups

    def copy(d):
        return pltpu.make_async_copy(
            w_hbm.at[pl.ds(cw * lax.rem(x + d, n), cw), :], w.at[pl.ds(cw * d, cw), :], sems.at[d]
        )

    for d in range(n):
        copy(d).start()
    for d in range(n):
        copy(d).wait()
        part = dot(normed_ref[:, d * cw : (d + 1) * cw], w[d * cw : (d + 1) * cw, :up])
        if d == 0:
            acc[...] = part
        else:
            acc[...] += part
    hidden = []
    for g in range(groups):
        u = acc[g * rows : (g + 1) * rows, :].astype(BF).astype(F32)
        c = (
            taps_ref[0:1] * pltpu.roll(u, 2, 0)
            + taps_ref[1:2] * pltpu.roll(u, 1, 0)
            + taps_ref[2:3] * u
        )[:count]
        gate = pltpu.roll(c, half, 1)[:, :half]
        hidden.append((silu(gate) * c[:, :half]).astype(BF))
    hidden = jnp.concatenate(hidden, axis=0)
    for d in range(n):
        t = nt_dot(hidden, w[d * cw : (d + 1) * cw, up:]).astype(BF)
        for g in range(groups):
            out_ref[d, g] = t[g * count : (g + 1) * count]


def call(kernel, out, *args, scratch=(), specs=None):
    vm = pl.BlockSpec(memory_space=pltpu.VMEM)
    return pl.pallas_call(
        kernel,
        out_shape=out,
        in_specs=specs or [vm] * len(args),
        out_specs=jax.tree.map(lambda _: vm, out),
        scratch_shapes=list(scratch),
    )(*args)


def moved(array, axis, by):
    n = lax.axis_size(axis)
    return lax.ppermute(array, axis, [(i, i + by) for i in range(n) if 0 <= i + by < n])


def from_peers(array):
    n = lax.axis_size("tp")
    return [array] + [
        lax.ppermute(array, "tp", [((i + d) % n, i) for i in range(n)]) for d in range(1, n)
    ]


def from_pair(array):
    return lax.ppermute(array, "grp_1", [(0, 1), (1, 0)])


def own_half(array, dim):
    n = array.shape[dim] // 2
    lo = lax.slice_in_dim(array, 0, n, axis=dim)
    hi = lax.slice_in_dim(array, n, 2 * n, axis=dim)
    return jnp.where(lax.axis_index("grp_1") == 0, lo, hi)


def entering(packed):
    partner = lax.ppermute(packed, "sp_1", [(0, 1), (1, 0)]).astype(F32)
    own = packed.astype(F32)
    second = lax.axis_index("sp_1") == 1

    def parts(p):
        p = p.astype(F32)
        return p[:DK], p[DK : DK + 1]

    first, later = jnp.where(second, partner, own), jnp.where(second, own, partner)
    s0, d0 = parts(first)
    s1, d1 = parts(later)

    def pack(s, d):
        return jnp.concatenate([s, jnp.broadcast_to(d, (HALO, d.shape[1]))], axis=0).astype(BF)

    chip = pack(d1 * s0 + s1, d0 * d1)
    n = lax.axis_size("sp_0")

    def window(p, shifts):
        got = [parts(moved(p, "sp_0", k)) for k in shifts if k < n]
        state, decay = got[-1]
        for s, d in got[-2::-1]:
            state = d * state + s
            decay = d * decay
        return state, decay

    state, decay = window(chip, (1, 2, 3, 4))
    if n > 4:
        before, _ = window(pack(state, decay), (4, 8, 12))
        state = state + decay * before
    return jnp.where(second, d0 * state + s0, state)


def on_device(
    residual_in,
    query_pre,
    forget_pre,
    value_pre,
    gate_pre,
    floor_gap,
    head_gain,
    out_weight,
    norm_gain,
    value_weight,
    gate_weight,
    value_taps,
    gate_taps,
    down_weight,
):
    count, cols = residual_in.shape
    width = query_pre.shape[1]
    rows = count + HALO
    n = lax.axis_size("tp")
    x = lax.axis_index("tp").astype(jnp.int32).reshape(1)
    share = jnp.concatenate(
        [own_half(value_weight, 1), own_half(gate_weight, 1), own_half(down_weight, 0).T], axis=1
    )
    gathered = lax.all_gather(share, SP, axis=0, tiled=True)

    tails = jnp.concatenate(
        [a[count - HALO :] for a in (query_pre, forget_pre, value_pre, gate_pre, residual_in)], axis=1
    )
    halo = moved(tails, SP, 1)
    sd = jax.ShapeDtypeStruct
    intra, qd, packed = call(
        local_kernel,
        (sd((rows, width), F32), sd((rows, width), BF), sd((DK + HALO, width), BF)),
        query_pre,
        forget_pre,
        value_pre,
        halo,
        floor_gap.reshape(1, width),
    )
    enter = entering(packed)
    head = call(
        head_kernel,
        sd((rows, width), BF),
        intra,
        qd,
        enter,
        gate_pre,
        halo[:, 3 * width : 4 * width],
        jnp.tile(head_gain, width // DK).reshape(1, width),
    )
    resid_halo = jnp.where(iota((HALO, cols), 0) < HALO - 2, 0.0, halo[:, 4 * width :].astype(F32))
    resid = jnp.concatenate([residual_in, resid_halo.astype(BF)], axis=0)
    resid = jnp.concatenate([resid, from_pair(resid)], axis=0)
    g0 = lax.reduce_precision(norm_gain, 8, 7)
    g1 = lax.reduce_precision(norm_gain - g0, 8, 7)
    g2 = norm_gain - g0 - g1
    gains = jnp.stack([g0, g1, g2] + [jnp.zeros_like(g0)] * (HALO - 3)).astype(BF)
    weights = from_peers(jnp.concatenate([out_weight, gains], axis=0))
    resids = from_peers(resid)
    heads = from_peers(jnp.concatenate([head, from_pair(head)], axis=0))
    hrows = out_weight.shape[0]
    vm = pl.BlockSpec(memory_space=pltpu.VMEM)
    sm = pl.BlockSpec(memory_space=pltpu.SMEM)
    hbm = pl.BlockSpec(memory_space=pl.ANY)
    normed, own = call(
        stream_kernel,
        (sd((2 * rows, n * cols), BF), sd((count, cols), F32)),
        x,
        *heads,
        *[w[:hrows] for w in weights],
        *resids,
        *[w[hrows:] for w in weights],
        specs=[sm] + [vm] * (4 * n),
    )
    taps = jnp.concatenate([own_half(value_taps, 1), own_half(gate_taps, 1)], axis=1)
    terms = call(
        mixer_kernel,
        sd((n, 2, count, cols), BF),
        x,
        normed,
        taps,
        gathered,
        specs=[sm, vm, vm, hbm],
        scratch=(
            pltpu.VMEM(gathered.shape, BF),
            pltpu.VMEM((2 * rows, taps.shape[1]), F32),
            pltpu.SemaphoreType.DMA((n,)),
        ),
    )
    total = own + terms[0, 0].astype(F32)
    for g in (1, 0):
        for d in range(n):
            if g or d:
                perm = [
                    (p * n + i, (p ^ g) * n + (i + d) % n) for p in range(2) for i in range(n)
                ]
                total = total + lax.ppermute(terms[d, g], PAIR, perm).astype(F32)
    return total.astype(BF)


def solution(mesh):
    groups, seq, tp = (mesh.shape[a] for a in ("grp", "sp", "tp"))
    finer = Mesh(
        mesh.devices.reshape(groups // 2, 2, seq // 2, 2, tp), (*GRP, *SP, "tp")
    )
    rows = P((*GRP, *SP), "tp")
    placed = (
        *[rows] * 5,
        P("tp"),
        P(),
        P(None, "tp"),
        P("tp"),
        P(SP, "tp"),
        P(SP, "tp"),
        P(None, "tp"),
        P(None, "tp"),
        P("tp", SP),
    )
    return jax.shard_map(on_device, mesh=finer, in_specs=placed, out_specs=rows, check_vma=False)
```

```python
import jax
import jax.numpy as jnp
from jax import lax
from jax.experimental import pallas as pl
from jax.experimental.pallas import tpu as pltpu
from jax.sharding import Mesh
from jax.sharding import PartitionSpec as P

BF = jnp.bfloat16
F32 = jnp.float32
EPS = 1e-06
DK = 64
SP = ("sp_0", "sp_1")
GRP = ("grp_0", "grp_1")
PAIR = ("grp_1", "tp")
HALO = 16
CH = 16


def silu(v):
    return v / (1.0 + jnp.exp(-v))


def nt_dot(a, b):
    return lax.dot_general(a, b, (((1,), (1,)), ((), ())), preferred_element_type=F32)


def tn_dot(a, b):
    return lax.dot_general(a, b, (((0,), (0,)), ((), ())), preferred_element_type=F32)


def dot(a, b):
    return jnp.dot(a, b, preferred_element_type=F32)


def iota(shape, dim):
    return lax.broadcasted_iota(jnp.int32, shape, dim)


def in_order(rows, halo):
    count = rows.shape[0]
    both = jnp.concatenate([rows.astype(F32), halo.astype(F32)], axis=0)
    row = iota(both.shape, 0)
    both = jnp.where((row >= count) & (row < count + HALO - 2), 0.0, both)
    return pltpu.roll(both, 2, 0)


def head_ones(width):
    a = iota((width, width), 0) // DK
    b = iota((width, width), 1) // DK
    return jnp.where(a == b, 1.0, 0.0).astype(BF)


def prep_kernel(p_ref, value_ref, gate_ref, down_ref, vt_ref, gt_ref, *refs):
    *parts, share_ref, tails_ref, taps_ref = refs
    first = p_ref[0] == 0
    up = value_ref.shape[1]
    half = up // 2

    def halves(v, g):
        v, g = v.astype(F32), g.astype(F32)
        lane = iota(v.shape, 1)
        vs = jnp.where(first, v, pltpu.roll(v, half, 1))
        gs = jnp.where(first, pltpu.roll(g, half, 1), g)
        return jnp.where(lane < half, vs, gs)

    share_ref[:, :up] = halves(value_ref[...], gate_ref[...]).astype(BF)
    d = down_ref[...].astype(F32)
    share_ref[:, up:] = jnp.where(first, d, pltpu.roll(d, half, 1))[:, :half].astype(BF)
    for i in range(vt_ref.shape[0]):
        v = jnp.broadcast_to(vt_ref[i : i + 1], (8, up))
        g = jnp.broadcast_to(gt_ref[i : i + 1], (8, up))
        taps_ref[8 * i : 8 * i + 8] = halves(v, g)
    at = 0
    for part in parts:
        count, width = part.shape
        tails_ref[:, at : at + width] = part[count - HALO :, :]
        at += width


def local_kernel(q_ref, f_ref, v_ref, halo_ref, gap_ref, res_ref, gain_ref, intra_ref, qd_ref, state_ref, ext_ref):
    count, width = q_ref.shape
    ext_ref[:count] = res_ref[...]
    gain = gain_ref[...]
    g0 = gain.astype(BF).astype(F32)
    g1 = (gain - g0).astype(BF).astype(F32)
    g2 = gain - g0 - g1
    tail = halo_ref[:, 4 * width :].astype(F32)
    place = iota(tail.shape, 0)
    tail = jnp.where(place < HALO - 2, 0.0, tail)
    for i, g in enumerate((g0, g1, g2)):
        tail = jnp.where(place == i, g, tail)
    ext_ref[count:] = tail.astype(BF)
    q = silu(in_order(q_ref[...], halo_ref[:, 0:width]))
    f = in_order(f_ref[...], halo_ref[:, width : 2 * width])
    v = in_order(v_ref[...], halo_ref[:, 2 * width : 3 * width])
    rows = q.shape[0]
    k = gap_ref[...] / (1.0 + jnp.exp(f))
    a = 1.0 - k
    la = jnp.log(a)
    row = iota(q.shape, 0)
    lane = iota((CH, width), 1)
    r = la
    step = 1
    while step < rows:
        r = r + jnp.where(row >= step, pltpu.roll(r, step, 0), 0.0)
        step *= 2
    ones = head_ones(width)
    inside = row % CH
    decay = jnp.ones_like(q)
    out = jnp.zeros_like(q)
    for j in range(CH):
        if j:
            decay = decay * (pltpu.roll(a, j - 1, 0) if j > 1 else a)
        kj = pltpu.roll(k, j, 0) if j else k
        vj = pltpu.roll(v, j, 0) if j else v
        term = jnp.where(inside >= j, q * decay * kj, 0.0)
        out = out + dot(term.astype(BF), ones) * vj
    pieces = [out[:CH]]
    vb = v.astype(BF)
    for i in range(1, rows // CH):
        lo = i * CH
        start = r[lo - 1 : lo]
        qi = q[lo : lo + CH] * jnp.exp(r[lo : lo + CH] - start)
        qi = jnp.concatenate([jnp.where(lane < DK, qi, 0.0), jnp.where(lane >= DK, qi, 0.0)], axis=0)
        ki = k[:lo] * jnp.exp(start - r[:lo])
        both = dot(nt_dot(qi.astype(BF), ki.astype(BF)).astype(BF), vb[:lo])
        pieces.append(out[lo : lo + CH] + jnp.where(lane < DK, both[:CH], both[CH:]))
    intra_ref[...] = jnp.concatenate(pieces, axis=0)
    qd_ref[...] = (q * jnp.exp(r)).astype(BF)
    last = r[count - 1 : count]
    kf = (k[:count] * jnp.exp(last - r[:count])).astype(BF)
    full = tn_dot(vb[:count], kf)
    half = iota((DK, width), 1)
    state_ref[:DK] = jnp.where(half < DK, full[:DK], full[DK:]).astype(BF)
    state_ref[DK:] = jnp.broadcast_to(jnp.exp(last), (HALO, width)).astype(BF)


def head_kernel(intra_ref, qd_ref, enter_ref, g_ref, halo_ref, gain_ref, out_ref):
    width = intra_ref.shape[1]
    half = iota((DK, width), 1)
    e = enter_ref[...]
    full = jnp.concatenate([jnp.where(half < DK, e, 0.0), jnp.where(half >= DK, e, 0.0)], axis=0)
    rec = intra_ref[...] + nt_dot(qd_ref[...], full.astype(BF))
    ones = head_ones(width)
    sq = rec * rec
    hi = sq.astype(BF)
    lo = (sq - hi.astype(F32)).astype(BF)
    mean = (dot(hi, ones) + dot(lo, ones)) * (1.0 / DK)
    gate = in_order(g_ref[...], halo_ref[:, 3 * width : 4 * width])
    gain = jnp.concatenate([gain_ref[...]] * (width // DK), axis=1)
    out = rec * lax.rsqrt(mean + EPS) * gain * silu(gate)
    out_ref[...] = pltpu.roll(out, out.shape[0] - 2, 0).astype(BF)


def stream_kernel(x_ref, *refs):
    n = (len(refs) - 2) // 3
    heads, weights, resid = (refs[i * n : (i + 1) * n] for i in range(3))
    normed_ref, own_ref = refs[3 * n :]
    count = own_ref.shape[0]
    x = x_ref[0]
    hw = heads[0].shape[1]
    cw = resid[0].shape[1]
    head = jnp.concatenate([h[...] for h in heads], axis=1)
    parts = []
    total = None
    for d in range(n):
        w = jnp.concatenate([weights[d][pl.ds(hw * lax.rem(x + e, n), hw), :] for e in range(n)], axis=0)
        s = resid[d][...].astype(F32) + dot(head, w)
        parts.append(s)
        sq = jnp.sum(s * s, axis=1, keepdims=True)
        total = sq if total is None else total + sq
    own_ref[...] = parts[0][: own_ref.shape[0]]
    scale = lax.rsqrt(total / (n * cw) + EPS)
    for d in range(n):
        g = resid[d][count : count + HALO].astype(F32)
        gain = g[0:1] + g[1:2] + g[2:3]
        normed_ref[:, d * cw : (d + 1) * cw] = (parts[d] * scale * gain).astype(BF)


def mixer_kernel(x_ref, normed_ref, taps_ref, w_hbm, *refs):
    *outs, w, acc, sems = refs
    groups = 2
    n = len(outs) // groups
    count = outs[0].shape[0]
    x = x_ref[0]
    cw = w.shape[0] // n
    up = taps_ref.shape[1]
    half = up // 2
    rows = acc.shape[0] // groups

    def copy(d):
        return pltpu.make_async_copy(
            w_hbm.at[pl.ds(cw * lax.rem(x + d, n), cw), :], w.at[pl.ds(cw * d, cw), :], sems.at[d]
        )

    for d in range(n):
        copy(d).start()
    for d in range(n):
        copy(d).wait()
        part = dot(normed_ref[:, d * cw : (d + 1) * cw], w[d * cw : (d + 1) * cw, :up])
        if d == 0:
            acc[...] = part
        else:
            acc[...] += part
    hidden = []
    for g in range(groups):
        u = acc[g * rows : (g + 1) * rows, :].astype(BF).astype(F32)
        c = (
            taps_ref[0:1] * pltpu.roll(u, 2, 0)
            + taps_ref[8:9] * pltpu.roll(u, 1, 0)
            + taps_ref[16:17] * u
        )[:count]
        gate = pltpu.roll(c, half, 1)[:, :half]
        hidden.append((silu(gate) * c[:, :half]).astype(BF))
    hidden = jnp.concatenate(hidden, axis=0)
    for d in range(n):
        t = nt_dot(hidden, w[d * cw : (d + 1) * cw, up:]).astype(BF)
        for g in range(groups):
            outs[d * groups + g][...] = t[g * count : (g + 1) * count]


def call(kernel, out, *args, scratch=(), specs=None):
    vm = pl.BlockSpec(memory_space=pltpu.VMEM)
    return pl.pallas_call(
        kernel,
        out_shape=out,
        in_specs=specs or [vm] * len(args),
        out_specs=jax.tree.map(lambda _: vm, out),
        scratch_shapes=list(scratch),
    )(*args)


def moved(array, axis, by):
    n = lax.axis_size(axis)
    return lax.ppermute(array, axis, [(i, i + by) for i in range(n) if 0 <= i + by < n])


def from_peers(array):
    n = lax.axis_size("tp")
    return [array] + [
        lax.ppermute(array, "tp", [((i + d) % n, i) for i in range(n)]) for d in range(1, n)
    ]


def from_pair(array):
    return lax.ppermute(array, "grp_1", [(0, 1), (1, 0)])


def entering(packed):
    partner = lax.ppermute(packed, "sp_1", [(0, 1), (1, 0)]).astype(F32)
    own = packed.astype(F32)
    second = lax.axis_index("sp_1") == 1

    def parts(p):
        p = p.astype(F32)
        return p[:DK], p[DK : DK + 1]

    first, later = jnp.where(second, partner, own), jnp.where(second, own, partner)
    s0, d0 = parts(first)
    s1, d1 = parts(later)

    def pack(s, d):
        return jnp.concatenate([s, jnp.broadcast_to(d, (HALO, d.shape[1]))], axis=0).astype(BF)

    chip = pack(d1 * s0 + s1, d0 * d1)
    n = lax.axis_size("sp_0")

    def window(p, shifts):
        got = [parts(moved(p, "sp_0", k)) for k in shifts if k < n]
        state, decay = got[-1]
        for s, d in got[-2::-1]:
            state = d * state + s
            decay = d * decay
        return state, decay

    state, decay = window(chip, (1, 2, 3, 4))
    if n > 4:
        before, _ = window(pack(state, decay), (4, 8, 12))
        state = state + decay * before
    return jnp.where(second, d0 * state + s0, state)


def on_device(
    residual_in,
    query_pre,
    forget_pre,
    value_pre,
    gate_pre,
    floor_gap,
    head_gain,
    out_weight,
    norm_gain,
    value_weight,
    gate_weight,
    value_taps,
    gate_taps,
    down_weight,
):
    count, cols = residual_in.shape
    width = query_pre.shape[1]
    rows = count + HALO
    n = lax.axis_size("tp")
    x = lax.axis_index("tp").astype(jnp.int32).reshape(1)
    p = lax.axis_index("grp_1").astype(jnp.int32).reshape(1)
    up = value_weight.shape[1]
    vm = pl.BlockSpec(memory_space=pltpu.VMEM)
    sm = pl.BlockSpec(memory_space=pltpu.SMEM)
    hbm = pl.BlockSpec(memory_space=pl.ANY)
    sd = jax.ShapeDtypeStruct
    share, tails, taps = call(
        prep_kernel,
        (
            sd((value_weight.shape[0], up + up // 2), BF),
            sd((HALO, 4 * width + cols), BF),
            sd((8 * value_taps.shape[0], up), F32),
        ),
        p,
        value_weight,
        gate_weight,
        down_weight.T,
        value_taps,
        gate_taps,
        query_pre,
        forget_pre,
        value_pre,
        gate_pre,
        residual_in,
        specs=[sm] + [vm] * 10,
    )
    gathered = lax.all_gather(share, SP, axis=0, tiled=True)
    weights = from_peers(out_weight)
    halo = moved(tails, SP, 1)
    intra, qd, packed, resid = call(
        local_kernel,
        (sd((rows, width), F32), sd((rows, width), BF), sd((DK + HALO, width), BF), sd((rows, cols), BF)),
        query_pre,
        forget_pre,
        value_pre,
        halo,
        floor_gap.reshape(1, width),
        residual_in,
        norm_gain.reshape(1, cols),
    )
    resids = from_peers(jnp.concatenate([resid, from_pair(resid)], axis=0))
    enter = entering(packed)
    head = call(
        head_kernel,
        sd((rows, width), BF),
        intra,
        qd,
        enter,
        gate_pre,
        halo,
        head_gain.reshape(1, DK),
    )
    heads = from_peers(jnp.concatenate([head, from_pair(head)], axis=0))
    normed, own = call(
        stream_kernel,
        (sd((2 * rows, n * cols), BF), sd((count, cols), F32)),
        x,
        *heads,
        *weights,
        *resids,
        specs=[sm] + [vm] * (3 * n),
    )
    terms = call(
        mixer_kernel,
        (sd((count, cols), BF),) * (2 * n),
        x,
        normed,
        taps,
        gathered,
        specs=[sm, vm, vm, hbm],
        scratch=(
            pltpu.VMEM(gathered.shape, BF),
            pltpu.VMEM((2 * rows, up), F32),
            pltpu.SemaphoreType.DMA((n,)),
        ),
    )
    total = own + terms[0].astype(F32)
    for g in (1, 0):
        for d in range(n):
            if g or d:
                perm = [
                    (p * n + i, (p ^ g) * n + (i + d) % n) for p in range(2) for i in range(n)
                ]
                total = total + lax.ppermute(terms[2 * d + g], PAIR, perm).astype(F32)
    return total.astype(BF)


def solution(mesh):
    groups, seq, tp = (mesh.shape[a] for a in ("grp", "sp", "tp"))
    finer = Mesh(
        mesh.devices.reshape(groups // 2, 2, seq // 2, 2, tp), (*GRP, *SP, "tp")
    )
    rows = P((*GRP, *SP), "tp")
    placed = (
        *[rows] * 5,
        P("tp"),
        P(),
        P(None, "tp"),
        P("tp"),
        P(SP, "tp"),
        P(SP, "tp"),
        P(None, "tp"),
        P(None, "tp"),
        P("tp", SP),
    )
    return jax.shard_map(on_device, mesh=finer, in_specs=placed, out_specs=rows, check_vma=False)
```

```python
import jax
import jax.numpy as jnp
from jax import lax
from jax.experimental import pallas as pl
from jax.experimental.pallas import tpu as pltpu
from jax.sharding import Mesh
from jax.sharding import PartitionSpec as P

BF = jnp.bfloat16
F32 = jnp.float32
EPS = 1e-06
DK = 64
SP = ("sp_0", "sp_1")
GRP = ("grp_0", "grp_1")
PAIR = ("grp_1", "tp")
HALO = 16
SPLIT = 2
CH = 16


def silu(v):
    return v / (1.0 + jnp.exp(-v))


def nt_dot(a, b):
    return lax.dot_general(a, b, (((1,), (1,)), ((), ())), preferred_element_type=F32)


def tn_dot(a, b):
    return lax.dot_general(a, b, (((0,), (0,)), ((), ())), preferred_element_type=F32)


def dot(a, b):
    return jnp.dot(a, b, preferred_element_type=F32)


def iota(shape, dim):
    return lax.broadcasted_iota(jnp.int32, shape, dim)


def in_order(rows, halo):
    count = rows.shape[0]
    both = jnp.concatenate([rows.astype(F32), halo.astype(F32)], axis=0)
    row = iota(both.shape, 0)
    both = jnp.where((row >= count) & (row < count + HALO - 2), 0.0, both)
    return pltpu.roll(both, 2, 0)


def head_ones(width):
    a = iota((width, width), 0) // DK
    b = iota((width, width), 1) // DK
    return jnp.where(a == b, 1.0, 0.0).astype(BF)


def prep_kernel(p_ref, value_ref, gate_ref, down_ref, vt_ref, gt_ref, *refs):
    *parts, share_ref, tails_ref, taps_ref = refs
    first = p_ref[0] == 0
    up = value_ref.shape[1]
    half = up // 2

    def halves(v, g):
        v, g = v.astype(F32), g.astype(F32)
        lane = iota(v.shape, 1)
        vs = jnp.where(first, v, pltpu.roll(v, half, 1))
        gs = jnp.where(first, pltpu.roll(g, half, 1), g)
        return jnp.where(lane < half, vs, gs)

    share_ref[:, :up] = halves(value_ref[...], gate_ref[...]).astype(BF)
    d = down_ref[...].astype(F32)
    share_ref[:, up:] = jnp.where(first, d, pltpu.roll(d, half, 1))[:, :half].astype(BF)
    for i in range(vt_ref.shape[0]):
        v = jnp.broadcast_to(vt_ref[i : i + 1], (8, up))
        g = jnp.broadcast_to(gt_ref[i : i + 1], (8, up))
        taps_ref[8 * i : 8 * i + 8] = halves(v, g)
    at = 0
    for part in parts:
        count, width = part.shape
        tails_ref[:, at : at + width] = part[count - HALO :, :]
        at += width


def local_kernel(q_ref, f_ref, v_ref, halo_ref, gap_ref, res_ref, gain_ref, intra_ref, qd_ref, state_ref, ext_ref):
    count, width = q_ref.shape
    ext_ref[:count] = res_ref[...]
    gain = gain_ref[...]
    g0 = gain.astype(BF).astype(F32)
    g1 = (gain - g0).astype(BF).astype(F32)
    g2 = gain - g0 - g1
    tail = halo_ref[:, 4 * width :].astype(F32)
    place = iota(tail.shape, 0)
    tail = jnp.where(place < HALO - 2, 0.0, tail)
    for i, g in enumerate((g0, g1, g2)):
        tail = jnp.where(place == i, g, tail)
    ext_ref[count:] = tail.astype(BF)
    q = silu(in_order(q_ref[...], halo_ref[:, 0:width]))
    f = in_order(f_ref[...], halo_ref[:, width : 2 * width])
    v = in_order(v_ref[...], halo_ref[:, 2 * width : 3 * width])
    rows = q.shape[0]
    k = gap_ref[...] / (1.0 + jnp.exp(f))
    a = 1.0 - k
    la = jnp.log(a)
    row = iota(q.shape, 0)
    lane = iota((CH, width), 1)
    r = la
    step = 1
    while step < rows:
        r = r + jnp.where(row >= step, pltpu.roll(r, step, 0), 0.0)
        step *= 2
    ones = head_ones(width)
    inside = row % CH
    decay = jnp.ones_like(q)
    out = jnp.zeros_like(q)
    for j in range(CH):
        if j:
            decay = decay * (pltpu.roll(a, j - 1, 0) if j > 1 else a)
        kj = pltpu.roll(k, j, 0) if j else k
        vj = pltpu.roll(v, j, 0) if j else v
        term = jnp.where(inside >= j, q * decay * kj, 0.0)
        out = out + dot(term.astype(BF), ones) * vj
    pieces = [out[:CH]]
    vb = v.astype(BF)
    for i in range(1, rows // CH):
        lo = i * CH
        start = r[lo - 1 : lo]
        qi = q[lo : lo + CH] * jnp.exp(r[lo : lo + CH] - start)
        qi = jnp.concatenate([jnp.where(lane < DK, qi, 0.0), jnp.where(lane >= DK, qi, 0.0)], axis=0)
        ki = k[:lo] * jnp.exp(start - r[:lo])
        both = dot(nt_dot(qi.astype(BF), ki.astype(BF)).astype(BF), vb[:lo])
        pieces.append(out[lo : lo + CH] + jnp.where(lane < DK, both[:CH], both[CH:]))
    intra_ref[...] = jnp.concatenate(pieces, axis=0)
    qd_ref[...] = (q * jnp.exp(r)).astype(BF)
    last = r[count - 1 : count]
    kf = (k[:count] * jnp.exp(last - r[:count])).astype(BF)
    full = tn_dot(vb[:count], kf)
    half = iota((DK, width), 1)
    state_ref[:DK] = jnp.where(half < DK, full[:DK], full[DK:]).astype(BF)
    state_ref[DK:] = jnp.broadcast_to(jnp.exp(last), (HALO, width)).astype(BF)


def head_kernel(intra_ref, qd_ref, enter_ref, g_ref, halo_ref, gain_ref, out_ref):
    width = intra_ref.shape[1]
    half = iota((DK, width), 1)
    e = enter_ref[...]
    full = jnp.concatenate([jnp.where(half < DK, e, 0.0), jnp.where(half >= DK, e, 0.0)], axis=0)
    rec = intra_ref[...] + nt_dot(qd_ref[...], full.astype(BF))
    ones = head_ones(width)
    sq = rec * rec
    hi = sq.astype(BF)
    lo = (sq - hi.astype(F32)).astype(BF)
    mean = (dot(hi, ones) + dot(lo, ones)) * (1.0 / DK)
    gate = in_order(g_ref[...], halo_ref[:, 3 * width : 4 * width])
    gain = jnp.concatenate([gain_ref[...]] * (width // DK), axis=1)
    out = rec * lax.rsqrt(mean + EPS) * gain * silu(gate)
    out_ref[...] = pltpu.roll(out, out.shape[0] - 2, 0).astype(BF)


def stream_kernel(x_ref, *refs):
    n = (len(refs) - 2) // 3
    heads, weights, resid = (refs[i * n : (i + 1) * n] for i in range(3))
    normed_ref, own_ref = refs[3 * n :]
    count = own_ref.shape[0]
    x = x_ref[0]
    hw = heads[0].shape[1]
    cw = resid[0].shape[1]
    head = jnp.concatenate([h[...] for h in heads], axis=1)
    parts = []
    total = None
    for d in range(n):
        w = jnp.concatenate([weights[d][pl.ds(hw * lax.rem(x + e, n), hw), :] for e in range(n)], axis=0)
        s = resid[d][...].astype(F32) + dot(head, w)
        parts.append(s)
        sq = jnp.sum(s * s, axis=1, keepdims=True)
        total = sq if total is None else total + sq
    own_ref[...] = parts[0][: own_ref.shape[0]]
    scale = lax.rsqrt(total / (n * cw) + EPS)
    for d in range(n):
        g = resid[d][count : count + HALO].astype(F32)
        gain = g[0:1] + g[1:2] + g[2:3]
        normed_ref[:, d * cw : (d + 1) * cw] = (parts[d] * scale * gain).astype(BF)


def mixer_kernel(x_ref, p_ref, normed_ref, taps_ref, w_hbm, out_ref, w, acc, sems):
    groups = 2
    n = out_ref.shape[0] // groups
    count = out_ref.shape[1]
    x = x_ref[0]
    p = p_ref[0]
    cw = w.shape[0] // n
    up = taps_ref.shape[1]
    half = up // 2
    rows = acc.shape[0] // groups

    def copy(d, i, lo, size, row, step):
        return pltpu.make_async_copy(
            w_hbm.at[pl.ds(cw * lax.rem(x + d, n) + row, step), pl.ds(lo, size)],
            w.at[pl.ds(cw * d + row, step), pl.ds(lo, size)],
            sems.at[i],
        )

    step = cw // SPLIT
    chunks = [(d, i) for d in range(n) for i in range(SPLIT)]
    ups = [copy(d, d * SPLIT + i, 0, up, i * step, step) for d, i in chunks]
    downs = [copy(d, n * SPLIT + d, up, half, 0, cw) for d in range(n)]
    for c in ups + downs:
        c.start()
    for (d, i), c in zip(chunks, ups):
        c.wait()
        at = d * cw + i * step
        part = dot(normed_ref[:, at : at + step], w[at : at + step, :up])
        if at == 0:
            acc[...] = part
        else:
            acc[...] += part
    hidden = []
    for g in range(groups):
        u = acc[g * rows : (g + 1) * rows, :].astype(BF).astype(F32)
        c = (
            taps_ref[0:1] * pltpu.roll(u, 2, 0)
            + taps_ref[8:9] * pltpu.roll(u, 1, 0)
            + taps_ref[16:17] * u
        )[:count]
        gate = pltpu.roll(c, half, 1)[:, :half]
        hidden.append((silu(gate) * c[:, :half]).astype(BF))
    hidden = jnp.concatenate(hidden, axis=0)
    for d in range(n):
        downs[d].wait()
        t = nt_dot(hidden, w[d * cw : (d + 1) * cw, up:]).astype(BF)
        for g in range(groups):
            place = (p if g == 0 else 1 - p) * n + lax.rem(x + d, n)
            out_ref[place] = t[g * count : (g + 1) * count]


def call(kernel, out, *args, scratch=(), specs=None):
    vm = pl.BlockSpec(memory_space=pltpu.VMEM)
    return pl.pallas_call(
        kernel,
        out_shape=out,
        in_specs=specs or [vm] * len(args),
        out_specs=jax.tree.map(lambda _: vm, out),
        scratch_shapes=list(scratch),
    )(*args)


def moved(array, axis, by):
    n = lax.axis_size(axis)
    return lax.ppermute(array, axis, [(i, i + by) for i in range(n) if 0 <= i + by < n])


def from_peers(array):
    n = lax.axis_size("tp")
    return [array] + [
        lax.ppermute(array, "tp", [((i + d) % n, i) for i in range(n)]) for d in range(1, n)
    ]


def from_pair(array):
    return lax.ppermute(array, "grp_1", [(0, 1), (1, 0)])


def entering(packed):
    partner = lax.ppermute(packed, "sp_1", [(0, 1), (1, 0)]).astype(F32)
    own = packed.astype(F32)
    second = lax.axis_index("sp_1") == 1

    def parts(p):
        p = p.astype(F32)
        return p[:DK], p[DK : DK + 1]

    first, later = jnp.where(second, partner, own), jnp.where(second, own, partner)
    s0, d0 = parts(first)
    s1, d1 = parts(later)

    def pack(s, d):
        return jnp.concatenate([s, jnp.broadcast_to(d, (HALO, d.shape[1]))], axis=0).astype(BF)

    chip = pack(d1 * s0 + s1, d0 * d1)
    n = lax.axis_size("sp_0")

    def window(p, shifts):
        got = [parts(moved(p, "sp_0", k)) for k in shifts if k < n]
        state, decay = got[-1]
        for s, d in got[-2::-1]:
            state = d * state + s
            decay = d * decay
        return state, decay

    state, decay = window(chip, (1, 2, 3, 4))
    if n > 4:
        before, _ = window(pack(state, decay), (4, 8, 12))
        state = state + decay * before
    return jnp.where(second, d0 * state + s0, state)


def on_device(
    residual_in,
    query_pre,
    forget_pre,
    value_pre,
    gate_pre,
    floor_gap,
    head_gain,
    out_weight,
    norm_gain,
    value_weight,
    gate_weight,
    value_taps,
    gate_taps,
    down_weight,
):
    count, cols = residual_in.shape
    width = query_pre.shape[1]
    rows = count + HALO
    n = lax.axis_size("tp")
    x = lax.axis_index("tp").astype(jnp.int32).reshape(1)
    p = lax.axis_index("grp_1").astype(jnp.int32).reshape(1)
    up = value_weight.shape[1]
    vm = pl.BlockSpec(memory_space=pltpu.VMEM)
    sm = pl.BlockSpec(memory_space=pltpu.SMEM)
    hbm = pl.BlockSpec(memory_space=pl.ANY)
    sd = jax.ShapeDtypeStruct
    share, tails, taps = call(
        prep_kernel,
        (
            sd((value_weight.shape[0], up + up // 2), BF),
            sd((HALO, 4 * width + cols), BF),
            sd((8 * value_taps.shape[0], up), F32),
        ),
        p,
        value_weight,
        gate_weight,
        down_weight.T,
        value_taps,
        gate_taps,
        query_pre,
        forget_pre,
        value_pre,
        gate_pre,
        residual_in,
        specs=[sm] + [vm] * 10,
    )
    gathered = lax.all_gather(share, SP, axis=0, tiled=True)
    weights = from_peers(out_weight)
    halo = moved(tails, SP, 1)
    intra, qd, packed, resid = call(
        local_kernel,
        (sd((rows, width), F32), sd((rows, width), BF), sd((DK + HALO, width), BF), sd((rows, cols), BF)),
        query_pre,
        forget_pre,
        value_pre,
        halo,
        floor_gap.reshape(1, width),
        residual_in,
        norm_gain.reshape(1, cols),
    )
    resids = from_peers(jnp.concatenate([resid, from_pair(resid)], axis=0))
    enter = entering(packed)
    head = call(
        head_kernel,
        sd((rows, width), BF),
        intra,
        qd,
        enter,
        gate_pre,
        halo,
        head_gain.reshape(1, DK),
    )
    heads = from_peers(jnp.concatenate([head, from_pair(head)], axis=0))
    normed, own = call(
        stream_kernel,
        (sd((2 * rows, n * cols), BF), sd((count, cols), F32)),
        x,
        *heads,
        *weights,
        *resids,
        specs=[sm] + [vm] * (3 * n),
    )
    terms = call(
        mixer_kernel,
        sd((2 * n, count, cols), BF),
        x,
        p,
        normed,
        taps,
        gathered,
        specs=[sm, sm, vm, vm, hbm],
        scratch=(
            pltpu.VMEM(gathered.shape, BF),
            pltpu.VMEM((2 * rows, up), F32),
            pltpu.SemaphoreType.DMA((n * SPLIT + n,)),
        ),
    )
    terms = lax.all_to_all(terms, PAIR, 0, 0, tiled=True)
    return (own + terms.astype(F32).sum(axis=0)).astype(BF)


def solution(mesh):
    groups, seq, tp = (mesh.shape[a] for a in ("grp", "sp", "tp"))
    finer = Mesh(
        mesh.devices.reshape(groups // 2, 2, seq // 2, 2, tp), (*GRP, *SP, "tp")
    )
    rows = P((*GRP, *SP), "tp")
    placed = (
        *[rows] * 5,
        P("tp"),
        P(),
        P(None, "tp"),
        P("tp"),
        P(SP, "tp"),
        P(SP, "tp"),
        P(None, "tp"),
        P(None, "tp"),
        P("tp", SP),
    )
    return jax.shard_map(on_device, mesh=finer, in_specs=placed, out_specs=rows, check_vma=False)
```

```python
import jax
import jax.numpy as jnp
from jax import lax
from jax.experimental import pallas as pl
from jax.experimental.pallas import tpu as pltpu
from jax.sharding import Mesh
from jax.sharding import PartitionSpec as P

BF = jnp.bfloat16
F32 = jnp.float32
EPS = 1e-06
DK = 64
SP = ("sp_0", "sp_1")
GRP = ("grp_0", "grp_1")
PAIR = ("grp_1", "tp")
HALO = 16
CH = 16


def silu(v):
    return v / (1.0 + jnp.exp(-v))


def nt_dot(a, b):
    return lax.dot_general(a, b, (((1,), (1,)), ((), ())), preferred_element_type=F32)


def tn_dot(a, b):
    return lax.dot_general(a, b, (((0,), (0,)), ((), ())), preferred_element_type=F32)


def dot(a, b):
    return jnp.dot(a, b, preferred_element_type=F32)


def iota(shape, dim):
    return lax.broadcasted_iota(jnp.int32, shape, dim)


def in_order(rows, halo):
    count = rows.shape[0]
    both = jnp.concatenate([rows.astype(F32), halo.astype(F32)], axis=0)
    row = iota(both.shape, 0)
    both = jnp.where((row >= count) & (row < count + HALO - 2), 0.0, both)
    return pltpu.roll(both, 2, 0)


def head_ones(width):
    a = iota((width, width), 0) // DK
    b = iota((width, width), 1) // DK
    return jnp.where(a == b, 1.0, 0.0).astype(BF)


def prep_kernel(p_ref, value_ref, gate_ref, down_ref, vt_ref, gt_ref, *refs):
    *parts, share_ref, tails_ref, taps_ref = refs
    first = p_ref[0] == 0
    up = value_ref.shape[1]
    half = up // 2

    def halves(v, g):
        v, g = v.astype(F32), g.astype(F32)
        lane = iota(v.shape, 1)
        vs = jnp.where(first, v, pltpu.roll(v, half, 1))
        gs = jnp.where(first, pltpu.roll(g, half, 1), g)
        return jnp.where(lane < half, vs, gs)

    share_ref[:, :up] = halves(value_ref[...], gate_ref[...]).astype(BF)
    d = down_ref[...].astype(F32)
    d = jnp.where(first, d, pltpu.roll(d, half, 1))[:, : share_ref.shape[1] - up]
    share_ref[:, up:] = d.astype(BF)
    for i in range(vt_ref.shape[0]):
        v = jnp.broadcast_to(vt_ref[i : i + 1], (8, up))
        g = jnp.broadcast_to(gt_ref[i : i + 1], (8, up))
        taps_ref[8 * i : 8 * i + 8] = halves(v, g)
    at = 0
    for part in parts:
        count, width = part.shape
        tails_ref[:, at : at + width] = part[count - HALO :, :]
        at += width


def local_kernel(q_ref, f_ref, v_ref, halo_ref, gap_ref, res_ref, gain_ref, intra_ref, qd_ref, state_ref, ext_ref):
    count, width = q_ref.shape
    ext_ref[:count] = res_ref[...]
    gain = gain_ref[...]
    g0 = gain.astype(BF).astype(F32)
    g1 = (gain - g0).astype(BF).astype(F32)
    g2 = gain - g0 - g1
    tail = halo_ref[:, 4 * width :].astype(F32)
    place = iota(tail.shape, 0)
    tail = jnp.where(place < HALO - 2, 0.0, tail)
    for i, g in enumerate((g0, g1, g2)):
        tail = jnp.where(place == i, g, tail)
    ext_ref[count:] = tail.astype(BF)
    q = silu(in_order(q_ref[...], halo_ref[:, 0:width]))
    f = in_order(f_ref[...], halo_ref[:, width : 2 * width])
    v = in_order(v_ref[...], halo_ref[:, 2 * width : 3 * width])
    rows = q.shape[0]
    k = gap_ref[...] / (1.0 + jnp.exp(f))
    a = 1.0 - k
    la = jnp.log(a)
    row = iota(q.shape, 0)
    lane = iota((CH, width), 1)
    r = la
    step = 1
    while step < rows:
        r = r + jnp.where(row >= step, pltpu.roll(r, step, 0), 0.0)
        step *= 2
    ones = head_ones(width)
    inside = row % CH
    decay = jnp.ones_like(q)
    out = jnp.zeros_like(q)
    for j in range(CH):
        if j:
            decay = decay * (pltpu.roll(a, j - 1, 0) if j > 1 else a)
        kj = pltpu.roll(k, j, 0) if j else k
        vj = pltpu.roll(v, j, 0) if j else v
        term = jnp.where(inside >= j, q * decay * kj, 0.0)
        out = out + dot(term.astype(BF), ones) * vj
    pieces = [out[:CH]]
    vb = v.astype(BF)
    for i in range(1, rows // CH):
        lo = i * CH
        start = r[lo - 1 : lo]
        qi = q[lo : lo + CH] * jnp.exp(r[lo : lo + CH] - start)
        qi = jnp.concatenate([jnp.where(lane < DK, qi, 0.0), jnp.where(lane >= DK, qi, 0.0)], axis=0)
        ki = k[:lo] * jnp.exp(start - r[:lo])
        both = dot(nt_dot(qi.astype(BF), ki.astype(BF)).astype(BF), vb[:lo])
        pieces.append(out[lo : lo + CH] + jnp.where(lane < DK, both[:CH], both[CH:]))
    intra_ref[...] = jnp.concatenate(pieces, axis=0)
    qd_ref[...] = (q * jnp.exp(r)).astype(BF)
    last = r[count - 1 : count]
    kf = (k[:count] * jnp.exp(last - r[:count])).astype(BF)
    full = tn_dot(vb[:count], kf)
    half = iota((DK, width), 1)
    state_ref[:DK] = jnp.where(half < DK, full[:DK], full[DK:]).astype(BF)
    state_ref[DK:] = jnp.broadcast_to(jnp.exp(last), (HALO, width)).astype(BF)


def head_kernel(intra_ref, qd_ref, enter_ref, g_ref, halo_ref, gain_ref, out_ref):
    width = intra_ref.shape[1]
    half = iota((DK, width), 1)
    e = enter_ref[...]
    full = jnp.concatenate([jnp.where(half < DK, e, 0.0), jnp.where(half >= DK, e, 0.0)], axis=0)
    rec = intra_ref[...] + nt_dot(qd_ref[...], full.astype(BF))
    ones = head_ones(width)
    sq = rec * rec
    hi = sq.astype(BF)
    lo = (sq - hi.astype(F32)).astype(BF)
    mean = (dot(hi, ones) + dot(lo, ones)) * (1.0 / DK)
    gate = in_order(g_ref[...], halo_ref[:, 3 * width : 4 * width])
    gain = jnp.concatenate([gain_ref[...]] * (width // DK), axis=1)
    out = rec * lax.rsqrt(mean + EPS) * gain * silu(gate)
    out_ref[...] = pltpu.roll(out, out.shape[0] - 2, 0).astype(BF)


def stream_kernel(x_ref, *refs):
    n = (len(refs) - 2) // 3
    heads, weights, resid = (refs[i * n : (i + 1) * n] for i in range(3))
    normed_ref, own_ref = refs[3 * n :]
    count = own_ref.shape[0]
    x = x_ref[0]
    hw = heads[0].shape[1]
    cw = resid[0].shape[1]
    head = jnp.concatenate([h[...] for h in heads], axis=1)
    parts = []
    total = None
    for d in range(n):
        w = jnp.concatenate([weights[d][pl.ds(hw * lax.rem(x + e, n), hw), :] for e in range(n)], axis=0)
        s = resid[d][...].astype(F32) + dot(head, w)
        parts.append(s)
        sq = jnp.sum(s * s, axis=1, keepdims=True)
        total = sq if total is None else total + sq
    own_ref[...] = parts[0][: own_ref.shape[0]]
    scale = lax.rsqrt(total / (n * cw) + EPS)
    for d in range(n):
        g = resid[d][count : count + HALO].astype(F32)
        gain = g[0:1] + g[1:2] + g[2:3]
        normed_ref[:, d * cw : (d + 1) * cw] = (parts[d] * scale * gain).astype(BF)


def mixer_kernel(at_ref, normed_ref, taps_ref, *refs):
    *pieces, out_ref, w, acc, sems = refs
    groups = 2
    n = out_ref.shape[0] // groups
    count = out_ref.shape[1]
    x, p, z, c = (at_ref[i] for i in range(4))
    cw = w.shape[0] // n
    up = taps_ref.shape[1]
    half = up // 2
    rows = acc.shape[0] // groups
    share = pieces[0].shape[0] // 2
    far = len(pieces) // 2
    chips = w.shape[0] // (2 * share)

    def place(ref, row, chip, core):
        to = 2 * share * chip + share * core
        block = lax.rem(lax.div(to, cw) + n - x, n)
        to = pl.multiple_of(block * cw + lax.rem(to, cw), share)
        pltpu.make_async_copy(
            ref.at[pl.ds(row, share), :], w.at[pl.ds(to, share), :], sems.at[block]
        ).start()

    place(pieces[0], 0, z, c)
    place(pieces[0], share, z, 1 - c)
    step = 1 - 2 * c
    for k in range(1, far + 1):
        own, other = pieces[k], pieces[far + k]
        below = lax.rem(z + chips - step * k, chips)
        above = lax.rem(z + chips + step * k, chips)
        place(own, 0, below, c)
        place(other, 0, above, 1 - c)
        if k < far:
            place(own, share, below, 1 - c)
            place(other, share, above, c)
    for d in range(n):
        block = w.at[pl.ds(cw * d, cw), :]
        pltpu.make_async_copy(block, block, sems.at[d]).wait()
        part = dot(normed_ref[:, d * cw : (d + 1) * cw], w[d * cw : (d + 1) * cw, :up])
        if d == 0:
            acc[...] = part
        else:
            acc[...] += part
    hidden = []
    for g in range(groups):
        u = acc[g * rows : (g + 1) * rows, :].astype(BF).astype(F32)
        c = (
            taps_ref[0:1] * pltpu.roll(u, 2, 0)
            + taps_ref[8:9] * pltpu.roll(u, 1, 0)
            + taps_ref[16:17] * u
        )[:count]
        gate = pltpu.roll(c, half, 1)[:, :half]
        hidden.append((silu(gate) * c[:, :half]).astype(BF))
    hidden = jnp.concatenate(hidden, axis=0)
    for d in range(n):
        t = nt_dot(hidden, w[d * cw : (d + 1) * cw, up : up + half]).astype(BF)
        for g in range(groups):
            to = (p if g == 0 else 1 - p) * n + lax.rem(x + d, n)
            out_ref[to] = t[g * count : (g + 1) * count]


def call(kernel, out, *args, scratch=(), specs=None):
    vm = pl.BlockSpec(memory_space=pltpu.VMEM)
    return pl.pallas_call(
        kernel,
        out_shape=out,
        in_specs=specs or [vm] * len(args),
        out_specs=jax.tree.map(lambda _: vm, out),
        scratch_shapes=list(scratch),
    )(*args)


def moved(array, axis, by):
    n = lax.axis_size(axis)
    return lax.ppermute(array, axis, [(i, i + by) for i in range(n) if 0 <= i + by < n])


def from_peers(array):
    n = lax.axis_size("tp")
    return [array] + [
        lax.ppermute(array, "tp", [((i + d) % n, i) for i in range(n)]) for d in range(1, n)
    ]


def from_pair(array):
    return lax.ppermute(array, "grp_1", [(0, 1), (1, 0)])


SWAP = [(0, 1), (1, 0)]


def passed_on(piece):
    n = lax.axis_size("sp_0")
    perm = [(2 * i + c, 2 * ((i + 1 - 2 * c) % n) + c) for i in range(n) for c in range(2)]
    return lax.ppermute(piece, SP, perm)


def step(pieces):
    pieces.append(passed_on(pieces[-1]))


def meet(pieces, *values):
    pieces[-1], *values = lax.optimization_barrier((pieces[-1], *values))
    return values


def state_of(packed):
    packed = packed.astype(F32)
    return packed[:DK], packed[DK : DK + 1]


def pack(state, decay):
    decay = jnp.broadcast_to(decay, (HALO, decay.shape[1]))
    return jnp.concatenate([state, decay], axis=0).astype(BF)


def earlier(packed, shifts):
    n = lax.axis_size("sp_0")
    return [moved(packed, "sp_0", k) for k in shifts if k < n]


def joined(got):
    got = [state_of(p) for p in got]
    state, decay = got[-1]
    for s, d in got[-2::-1]:
        state = d * state + s
        decay = d * decay
    return state, decay


def on_device(
    residual_in,
    query_pre,
    forget_pre,
    value_pre,
    gate_pre,
    floor_gap,
    head_gain,
    out_weight,
    norm_gain,
    value_weight,
    gate_weight,
    value_taps,
    gate_taps,
    down_weight,
):
    count, cols = residual_in.shape
    width = query_pre.shape[1]
    rows = count + HALO
    n = lax.axis_size("tp")
    x = lax.axis_index("tp").astype(jnp.int32).reshape(1)
    p = lax.axis_index("grp_1").astype(jnp.int32).reshape(1)
    up = value_weight.shape[1]
    vm = pl.BlockSpec(memory_space=pltpu.VMEM)
    sm = pl.BlockSpec(memory_space=pltpu.SMEM)
    hbm = pl.BlockSpec(memory_space=pl.ANY)
    sd = jax.ShapeDtypeStruct
    share, tails, taps = call(
        prep_kernel,
        (
            sd((value_weight.shape[0], -(-3 * up // 256) * 128), BF),
            sd((HALO, 4 * width + cols), BF),
            sd((8 * value_taps.shape[0], up), F32),
        ),
        p,
        value_weight,
        gate_weight,
        down_weight.T,
        value_taps,
        gate_taps,
        query_pre,
        forget_pre,
        value_pre,
        gate_pre,
        residual_in,
        specs=[sm] + [vm] * 10,
    )
    halo = moved(tails, SP, 1)
    other = lax.ppermute(share, "sp_1", SWAP)
    halo, other = lax.optimization_barrier((halo, other))
    pieces = [jnp.concatenate([share, other], axis=0)]
    weights = from_peers(out_weight)
    intra, qd, packed, resid = call(
        local_kernel,
        (sd((rows, width), F32), sd((rows, width), BF), sd((DK + HALO, width), BF), sd((rows, cols), BF)),
        query_pre,
        forget_pre,
        value_pre,
        halo,
        floor_gap.reshape(1, width),
        residual_in,
        norm_gain.reshape(1, cols),
    )
    step(pieces)
    resid_pair = from_pair(resid)
    second = lax.axis_index("sp_1") == 1
    partner = lax.ppermute(packed, "sp_1", SWAP)
    s0, d0 = state_of(jnp.where(second, partner, packed))
    s1, d1 = state_of(jnp.where(second, packed, partner))
    chip, resid_pair = meet(pieces, pack(d1 * s0 + s1, d0 * d1), resid_pair)
    step(pieces)
    got = earlier(chip, (1, 2, 3, 4))
    got[0], *weights[1:] = meet(pieces, got[0], *weights[1:])
    step(pieces)
    swapped = [lax.ppermute(piece, "sp_1", SWAP) for piece in pieces[1:3]]
    state, decay, *swapped = meet(pieces, *joined(got), *swapped)
    step(pieces)
    got = earlier(pack(state, decay), (4, 8, 12))
    resids = from_peers(jnp.concatenate([resid, resid_pair], axis=0))
    (got[0],) = meet(pieces, got[0])
    step(pieces)
    state = state + decay * joined(got)[0]
    swapped += [lax.ppermute(piece, "sp_1", SWAP) for piece in pieces[3:5]]
    state, *swapped = meet(pieces, state, *swapped)
    enter = jnp.where(second, d0 * state + s0, state)
    head = call(
        head_kernel,
        sd((rows, width), BF),
        intra,
        qd,
        enter,
        gate_pre,
        halo,
        head_gain.reshape(1, DK),
    )
    step(pieces)
    pair, *resids[1:] = meet(pieces, from_pair(head), *resids[1:])
    step(pieces)
    heads = from_peers(jnp.concatenate([head, pair], axis=0))
    swapped += [lax.ppermute(piece, "sp_1", SWAP) for piece in pieces[5:7]]
    *heads[1:], s1, s2 = meet(pieces, *heads[1:], *swapped[-2:])
    swapped[-2:] = [s1, s2]
    pieces.append(passed_on(pieces[-1][: share.shape[0]]))
    pieces += swapped + [lax.ppermute(piece, "sp_1", SWAP) for piece in pieces[7:9]]
    normed, own = call(
        stream_kernel,
        (sd((2 * rows, n * cols), BF), sd((count, cols), F32)),
        x,
        *heads,
        *weights,
        *resids,
        specs=[sm] + [vm] * (3 * n),
    )
    at = jnp.stack([lax.axis_index(a) for a in ("tp", "grp_1", "sp_0", "sp_1")]).astype(jnp.int32)
    terms = call(
        mixer_kernel,
        sd((2 * n, count, cols), BF),
        at,
        normed,
        taps,
        *pieces,
        specs=[sm, vm, vm] + [hbm] * len(pieces),
        scratch=(
            pltpu.VMEM((n * cols, share.shape[1]), BF),
            pltpu.VMEM((2 * rows, up), F32),
            pltpu.SemaphoreType.DMA((n,)),
        ),
    )
    terms = lax.all_to_all(terms, PAIR, 0, 0, tiled=True)
    return (own + terms.astype(F32).sum(axis=0)).astype(BF)


def solution(mesh):
    groups, seq, tp = (mesh.shape[a] for a in ("grp", "sp", "tp"))
    finer = Mesh(
        mesh.devices.reshape(groups // 2, 2, seq // 2, 2, tp), (*GRP, *SP, "tp")
    )
    rows = P((*GRP, *SP), "tp")
    placed = (
        *[rows] * 5,
        P("tp"),
        P(),
        P(None, "tp"),
        P("tp"),
        P(SP, "tp"),
        P(SP, "tp"),
        P(None, "tp"),
        P(None, "tp"),
        P("tp", SP),
    )
    return jax.shard_map(on_device, mesh=finer, in_specs=placed, out_specs=rows, check_vma=False)
```

```python
import jax
import jax.numpy as jnp
from jax import lax
from jax.experimental import pallas as pl
from jax.experimental.pallas import tpu as pltpu
from jax.sharding import Mesh
from jax.sharding import PartitionSpec as P

BF = jnp.bfloat16
F32 = jnp.float32
EPS = 1e-06
DK = 64
SP = ("sp_0", "sp_1")
GRP = ("grp_0", "grp_1")
PAIR = ("grp_1", "tp")
HALO = 16
CH = 16


def silu(v):
    return v / (1.0 + jnp.exp(-v))


def nt_dot(a, b):
    return lax.dot_general(a, b, (((1,), (1,)), ((), ())), preferred_element_type=F32)


def tn_dot(a, b):
    return lax.dot_general(a, b, (((0,), (0,)), ((), ())), preferred_element_type=F32)


def dot(a, b):
    return jnp.dot(a, b, preferred_element_type=F32)


def iota(shape, dim):
    return lax.broadcasted_iota(jnp.int32, shape, dim)


def in_order(rows, halo):
    count = rows.shape[0]
    both = jnp.concatenate([rows.astype(F32), halo.astype(F32)], axis=0)
    row = iota(both.shape, 0)
    both = jnp.where((row >= count) & (row < count + HALO - 2), 0.0, both)
    return pltpu.roll(both, 2, 0)


def head_ones(width):
    a = iota((width, width), 0) // DK
    b = iota((width, width), 1) // DK
    return jnp.where(a == b, 1.0, 0.0).astype(BF)


def halves(first, v, g):
    v, g = v.astype(F32), g.astype(F32)
    half = v.shape[1] // 2
    lane = iota(v.shape, 1)
    vs = jnp.where(first, v, pltpu.roll(v, half, 1))
    gs = jnp.where(first, pltpu.roll(g, half, 1), g)
    return jnp.where(lane < half, vs, gs)


def share_kernel(p_ref, value_ref, gate_ref, down_ref, share_ref):
    first = p_ref[0] == 0
    up = value_ref.shape[1]
    half = up // 2
    share_ref[:, :up] = halves(first, value_ref[...], gate_ref[...]).astype(BF)
    d = down_ref[...].astype(F32)
    share_ref[:, up:] = jnp.where(first, d, pltpu.roll(d, half, 1))[:, :half].astype(BF)


def prep_kernel(p_ref, vt_ref, gt_ref, *refs):
    *parts, tails_ref, taps_ref = refs
    first = p_ref[0] == 0
    up = vt_ref.shape[1]
    for i in range(vt_ref.shape[0]):
        v = jnp.broadcast_to(vt_ref[i : i + 1], (8, up))
        g = jnp.broadcast_to(gt_ref[i : i + 1], (8, up))
        taps_ref[8 * i : 8 * i + 8] = halves(first, v, g)
    at = 0
    for part in parts:
        count, width = part.shape
        tails_ref[:, at : at + width] = part[count - HALO :, :]
        at += width


def local_kernel(q_ref, f_ref, v_ref, halo_ref, gap_ref, res_ref, gain_ref, intra_ref, qd_ref, state_ref, ext_ref):
    count, width = q_ref.shape
    ext_ref[:count] = res_ref[...]
    gain = gain_ref[...]
    g0 = gain.astype(BF).astype(F32)
    g1 = (gain - g0).astype(BF).astype(F32)
    g2 = gain - g0 - g1
    tail = halo_ref[:, 4 * width :].astype(F32)
    place = iota(tail.shape, 0)
    tail = jnp.where(place < HALO - 2, 0.0, tail)
    for i, g in enumerate((g0, g1, g2)):
        tail = jnp.where(place == i, g, tail)
    ext_ref[count:] = tail.astype(BF)
    q = silu(in_order(q_ref[...], halo_ref[:, 0:width]))
    f = in_order(f_ref[...], halo_ref[:, width : 2 * width])
    v = in_order(v_ref[...], halo_ref[:, 2 * width : 3 * width])
    rows = q.shape[0]
    k = gap_ref[...] / (1.0 + jnp.exp(f))
    a = 1.0 - k
    la = jnp.log(a)
    row = iota(q.shape, 0)
    lane = iota((CH, width), 1)
    r = la
    step = 1
    while step < rows:
        r = r + jnp.where(row >= step, pltpu.roll(r, step, 0), 0.0)
        step *= 2
    ones = head_ones(width)
    inside = row % CH
    decay = jnp.ones_like(q)
    out = jnp.zeros_like(q)
    for j in range(CH):
        if j:
            decay = decay * (pltpu.roll(a, j - 1, 0) if j > 1 else a)
        kj = pltpu.roll(k, j, 0) if j else k
        vj = pltpu.roll(v, j, 0) if j else v
        term = jnp.where(inside >= j, q * decay * kj, 0.0)
        out = out + dot(term.astype(BF), ones) * vj
    pieces = [out[:CH]]
    vb = v.astype(BF)
    for i in range(1, rows // CH):
        lo = i * CH
        start = r[lo - 1 : lo]
        qi = q[lo : lo + CH] * jnp.exp(r[lo : lo + CH] - start)
        qi = jnp.concatenate([jnp.where(lane < DK, qi, 0.0), jnp.where(lane >= DK, qi, 0.0)], axis=0)
        ki = k[:lo] * jnp.exp(start - r[:lo])
        both = dot(nt_dot(qi.astype(BF), ki.astype(BF)).astype(BF), vb[:lo])
        pieces.append(out[lo : lo + CH] + jnp.where(lane < DK, both[:CH], both[CH:]))
    intra_ref[...] = jnp.concatenate(pieces, axis=0)
    qd_ref[...] = (q * jnp.exp(r)).astype(BF)
    last = r[count - 1 : count]
    kf = (k[:count] * jnp.exp(last - r[:count])).astype(BF)
    full = tn_dot(vb[:count], kf)
    half = iota((DK, width), 1)
    state_ref[:DK] = jnp.where(half < DK, full[:DK], full[DK:]).astype(BF)
    state_ref[DK:] = jnp.broadcast_to(jnp.exp(last), (HALO, width)).astype(BF)


def head_kernel(intra_ref, qd_ref, enter_ref, g_ref, halo_ref, gain_ref, out_ref):
    width = intra_ref.shape[1]
    half = iota((DK, width), 1)
    e = enter_ref[...]
    full = jnp.concatenate([jnp.where(half < DK, e, 0.0), jnp.where(half >= DK, e, 0.0)], axis=0)
    rec = intra_ref[...] + nt_dot(qd_ref[...], full.astype(BF))
    ones = head_ones(width)
    sq = rec * rec
    hi = sq.astype(BF)
    lo = (sq - hi.astype(F32)).astype(BF)
    mean = (dot(hi, ones) + dot(lo, ones)) * (1.0 / DK)
    gate = in_order(g_ref[...], halo_ref[:, 3 * width : 4 * width])
    gain = jnp.concatenate([gain_ref[...]] * (width // DK), axis=1)
    out = rec * lax.rsqrt(mean + EPS) * gain * silu(gate)
    out_ref[...] = pltpu.roll(out, out.shape[0] - 2, 0).astype(BF)


def stream_kernel(x_ref, *refs):
    n = (len(refs) - 2) // 3
    heads, weights, resid = (refs[i * n : (i + 1) * n] for i in range(3))
    normed_ref, own_ref = refs[3 * n :]
    count = own_ref.shape[0]
    x = x_ref[0]
    hw = heads[0].shape[1]
    cw = resid[0].shape[1]
    head = jnp.concatenate([h[...] for h in heads], axis=1)
    parts = []
    total = None
    for d in range(n):
        w = jnp.concatenate([weights[d][pl.ds(hw * lax.rem(x + e, n), hw), :] for e in range(n)], axis=0)
        s = resid[d][...].astype(F32) + dot(head, w)
        parts.append(s)
        sq = jnp.sum(s * s, axis=1, keepdims=True)
        total = sq if total is None else total + sq
    own_ref[...] = parts[0][: own_ref.shape[0]]
    scale = lax.rsqrt(total / (n * cw) + EPS)
    for d in range(n):
        g = resid[d][count : count + HALO].astype(F32)
        gain = g[0:1] + g[1:2] + g[2:3]
        normed_ref[:, d * cw : (d + 1) * cw] = (parts[d] * scale * gain).astype(BF)


def mixer_kernel(x_ref, p_ref, normed_ref, taps_ref, w_hbm, out_ref, w, acc, sems):
    groups = 2
    n = out_ref.shape[0] // groups
    count = out_ref.shape[1]
    x = x_ref[0]
    p = p_ref[0]
    cw = w.shape[0] // n
    up = taps_ref.shape[1]
    half = up // 2
    rows = acc.shape[0] // groups

    def copy(d):
        return pltpu.make_async_copy(
            w_hbm.at[pl.ds(cw * lax.rem(x + d, n), cw), :], w.at[pl.ds(cw * d, cw), :], sems.at[d]
        )

    for d in range(n):
        copy(d).start()
    for d in range(n):
        copy(d).wait()
        part = dot(normed_ref[:, d * cw : (d + 1) * cw], w[d * cw : (d + 1) * cw, :up])
        if d == 0:
            acc[...] = part
        else:
            acc[...] += part
    hidden = []
    for g in range(groups):
        u = acc[g * rows : (g + 1) * rows, :].astype(BF).astype(F32)
        c = (
            taps_ref[0:1] * pltpu.roll(u, 2, 0)
            + taps_ref[8:9] * pltpu.roll(u, 1, 0)
            + taps_ref[16:17] * u
        )[:count]
        gate = pltpu.roll(c, half, 1)[:, :half]
        hidden.append((silu(gate) * c[:, :half]).astype(BF))
    hidden = jnp.concatenate(hidden, axis=0)
    for d in range(n):
        t = nt_dot(hidden, w[d * cw : (d + 1) * cw, up:]).astype(BF)
        for g in range(groups):
            place = (p if g == 0 else 1 - p) * n + lax.rem(x + d, n)
            out_ref[place] = t[g * count : (g + 1) * count]


def call(kernel, out, *args, scratch=(), specs=None):
    vm = pl.BlockSpec(memory_space=pltpu.VMEM)
    return pl.pallas_call(
        kernel,
        out_shape=out,
        in_specs=specs or [vm] * len(args),
        out_specs=jax.tree.map(lambda _: vm, out),
        scratch_shapes=list(scratch),
    )(*args)


def moved(array, axis, by):
    n = lax.axis_size(axis)
    return lax.ppermute(array, axis, [(i, i + by) for i in range(n) if 0 <= i + by < n])


def from_peers(array):
    n = lax.axis_size("tp")
    return [array] + [
        lax.ppermute(array, "tp", [((i + d) % n, i) for i in range(n)]) for d in range(1, n)
    ]


def from_pair(array):
    return lax.ppermute(array, "grp_1", [(0, 1), (1, 0)])


def entering(packed):
    partner = lax.ppermute(packed, "sp_1", [(0, 1), (1, 0)]).astype(F32)
    own = packed.astype(F32)
    second = lax.axis_index("sp_1") == 1

    def parts(p):
        p = p.astype(F32)
        return p[:DK], p[DK : DK + 1]

    first, later = jnp.where(second, partner, own), jnp.where(second, own, partner)
    s0, d0 = parts(first)
    s1, d1 = parts(later)

    def pack(s, d):
        return jnp.concatenate([s, jnp.broadcast_to(d, (HALO, d.shape[1]))], axis=0).astype(BF)

    chip = pack(d1 * s0 + s1, d0 * d1)
    n = lax.axis_size("sp_0")

    def before(p, shift):
        return parts(moved(p, "sp_0", shift))

    (state, decay), (s, d) = before(chip, 1), before(chip, 2)
    state, decay = state + decay * s, decay * d
    shift = 2
    while shift < n:
        s, d = before(pack(state, decay), shift)
        state, decay = state + decay * s, decay * d
        shift *= 2
    return jnp.where(second, d0 * state + s0, state)


def on_device(
    residual_in,
    query_pre,
    forget_pre,
    value_pre,
    gate_pre,
    floor_gap,
    head_gain,
    out_weight,
    norm_gain,
    value_weight,
    gate_weight,
    value_taps,
    gate_taps,
    down_weight,
):
    count, cols = residual_in.shape
    width = query_pre.shape[1]
    rows = count + HALO
    n = lax.axis_size("tp")
    x = lax.axis_index("tp").astype(jnp.int32).reshape(1)
    p = lax.axis_index("grp_1").astype(jnp.int32).reshape(1)
    up = value_weight.shape[1]
    vm = pl.BlockSpec(memory_space=pltpu.VMEM)
    sm = pl.BlockSpec(memory_space=pltpu.SMEM)
    hbm = pl.BlockSpec(memory_space=pl.ANY)
    sd = jax.ShapeDtypeStruct
    share = call(
        share_kernel,
        sd((value_weight.shape[0], up + up // 2), BF),
        p,
        value_weight,
        gate_weight,
        down_weight.T,
        specs=[sm] + [vm] * 3,
    )
    share, p = lax.optimization_barrier((share, p))
    gathered = lax.all_gather(share, SP, axis=0, tiled=True)
    tails, taps = call(
        prep_kernel,
        (sd((HALO, 4 * width + cols), BF), sd((8 * value_taps.shape[0], up), F32)),
        p,
        value_taps,
        gate_taps,
        query_pre,
        forget_pre,
        value_pre,
        gate_pre,
        residual_in,
        specs=[sm] + [vm] * 7,
    )
    weights = from_peers(out_weight)
    halo = moved(tails, SP, 1)
    intra, qd, packed, resid = call(
        local_kernel,
        (sd((rows, width), F32), sd((rows, width), BF), sd((DK + HALO, width), BF), sd((rows, cols), BF)),
        query_pre,
        forget_pre,
        value_pre,
        halo,
        floor_gap.reshape(1, width),
        residual_in,
        norm_gain.reshape(1, cols),
    )
    resids = from_peers(jnp.concatenate([resid, from_pair(resid)], axis=0))
    enter = entering(packed)
    head = call(
        head_kernel,
        sd((rows, width), BF),
        intra,
        qd,
        enter,
        gate_pre,
        halo,
        head_gain.reshape(1, DK),
    )
    heads = from_peers(jnp.concatenate([head, from_pair(head)], axis=0))
    normed, own = call(
        stream_kernel,
        (sd((2 * rows, n * cols), BF), sd((count, cols), F32)),
        x,
        *heads,
        *weights,
        *resids,
        specs=[sm] + [vm] * (3 * n),
    )
    terms = call(
        mixer_kernel,
        sd((2 * n, count, cols), BF),
        x,
        p,
        normed,
        taps,
        gathered,
        specs=[sm, sm, vm, vm, hbm],
        scratch=(
            pltpu.VMEM(gathered.shape, BF),
            pltpu.VMEM((2 * rows, up), F32),
            pltpu.SemaphoreType.DMA((n,)),
        ),
    )
    terms = lax.all_to_all(terms, PAIR, 0, 0, tiled=True)
    return (own + terms.astype(F32).sum(axis=0)).astype(BF)


def solution(mesh):
    groups, seq, tp = (mesh.shape[a] for a in ("grp", "sp", "tp"))
    finer = Mesh(
        mesh.devices.reshape(groups // 2, 2, seq // 2, 2, tp), (*GRP, *SP, "tp")
    )
    rows = P((*GRP, *SP), "tp")
    placed = (
        *[rows] * 5,
        P("tp"),
        P(),
        P(None, "tp"),
        P("tp"),
        P(SP, "tp"),
        P(SP, "tp"),
        P(None, "tp"),
        P(None, "tp"),
        P("tp", SP),
    )
    return jax.shard_map(on_device, mesh=finer, in_specs=placed, out_specs=rows, check_vma=False)
```

```python
import jax
import jax.numpy as jnp
from jax import lax
from jax.experimental import pallas as pl
from jax.experimental.pallas import tpu as pltpu
from jax.sharding import Mesh
from jax.sharding import PartitionSpec as P

BF = jnp.bfloat16
F32 = jnp.float32
EPS = 1e-06
DK = 64
SP = ("sp_0", "sp_1")
GRP = ("grp_0", "grp_1")
PAIR = ("grp_1", "tp")
HALO = 16
CH = 16


def silu(v):
    return v / (1.0 + jnp.exp(-v))


def nt_dot(a, b):
    return lax.dot_general(a, b, (((1,), (1,)), ((), ())), preferred_element_type=F32)


def tn_dot(a, b):
    return lax.dot_general(a, b, (((0,), (0,)), ((), ())), preferred_element_type=F32)


def dot(a, b):
    return jnp.dot(a, b, preferred_element_type=F32)


def iota(shape, dim):
    return lax.broadcasted_iota(jnp.int32, shape, dim)


def in_order(rows, halo):
    count = rows.shape[0]
    both = jnp.concatenate([rows.astype(F32), halo.astype(F32)], axis=0)
    row = iota(both.shape, 0)
    both = jnp.where((row >= count) & (row < count + HALO - 2), 0.0, both)
    return pltpu.roll(both, 2, 0)


def head_ones(width):
    a = iota((width, width), 0) // DK
    b = iota((width, width), 1) // DK
    return jnp.where(a == b, 1.0, 0.0).astype(BF)


def halves(first, v, g):
    v, g = v.astype(F32), g.astype(F32)
    half = v.shape[1] // 2
    lane = iota(v.shape, 1)
    vs = jnp.where(first, v, pltpu.roll(v, half, 1))
    gs = jnp.where(first, pltpu.roll(g, half, 1), g)
    return jnp.where(lane < half, vs, gs)


def share_kernel(p_ref, value_ref, gate_ref, down_ref, share_ref):
    first = p_ref[0] == 0
    up = value_ref.shape[1]
    half = up // 2
    share_ref[:, :up] = halves(first, value_ref[...], gate_ref[...]).astype(BF)
    d = down_ref[...].astype(F32)
    share_ref[:, up:] = jnp.where(first, d, pltpu.roll(d, half, 1))[:, :half].astype(BF)


def prep_kernel(p_ref, vt_ref, gt_ref, *refs):
    *parts, tails_ref, taps_ref = refs
    first = p_ref[0] == 0
    up = vt_ref.shape[1]
    for i in range(vt_ref.shape[0]):
        v = jnp.broadcast_to(vt_ref[i : i + 1], (8, up))
        g = jnp.broadcast_to(gt_ref[i : i + 1], (8, up))
        taps_ref[8 * i : 8 * i + 8] = halves(first, v, g)
    at = 0
    for part in parts:
        count, width = part.shape
        tails_ref[:, at : at + width] = part[count - HALO :, :]
        at += width


def local_kernel(q_ref, f_ref, v_ref, halo_ref, gap_ref, res_ref, gain_ref, intra_ref, qd_ref, state_ref, ext_ref):
    count, width = q_ref.shape
    ext_ref[:count] = res_ref[...]
    gain = gain_ref[...]
    g0 = gain.astype(BF).astype(F32)
    g1 = (gain - g0).astype(BF).astype(F32)
    g2 = gain - g0 - g1
    tail = halo_ref[:, 4 * width :].astype(F32)
    place = iota(tail.shape, 0)
    tail = jnp.where(place < HALO - 2, 0.0, tail)
    for i, g in enumerate((g0, g1, g2)):
        tail = jnp.where(place == i, g, tail)
    ext_ref[count:] = tail.astype(BF)
    q = silu(in_order(q_ref[...], halo_ref[:, 0:width]))
    f = in_order(f_ref[...], halo_ref[:, width : 2 * width])
    v = in_order(v_ref[...], halo_ref[:, 2 * width : 3 * width])
    rows = q.shape[0]
    k = gap_ref[...] / (1.0 + jnp.exp(f))
    a = 1.0 - k
    la = jnp.log(a)
    row = iota(q.shape, 0)
    lane = iota((CH, width), 1)
    r = la
    step = 1
    while step < rows:
        r = r + jnp.where(row >= step, pltpu.roll(r, step, 0), 0.0)
        step *= 2
    ones = head_ones(width)
    inside = row % CH
    decay = jnp.ones_like(q)
    out = jnp.zeros_like(q)
    for j in range(CH):
        if j:
            decay = decay * (pltpu.roll(a, j - 1, 0) if j > 1 else a)
        kj = pltpu.roll(k, j, 0) if j else k
        vj = pltpu.roll(v, j, 0) if j else v
        term = jnp.where(inside >= j, q * decay * kj, 0.0)
        out = out + dot(term.astype(BF), ones) * vj
    pieces = [out[:CH]]
    vb = v.astype(BF)
    for i in range(1, rows // CH):
        lo = i * CH
        start = r[lo - 1 : lo]
        qi = q[lo : lo + CH] * jnp.exp(r[lo : lo + CH] - start)
        qi = jnp.concatenate([jnp.where(lane < DK, qi, 0.0), jnp.where(lane >= DK, qi, 0.0)], axis=0)
        ki = k[:lo] * jnp.exp(start - r[:lo])
        both = dot(nt_dot(qi.astype(BF), ki.astype(BF)).astype(BF), vb[:lo])
        pieces.append(out[lo : lo + CH] + jnp.where(lane < DK, both[:CH], both[CH:]))
    intra_ref[...] = jnp.concatenate(pieces, axis=0)
    qd_ref[...] = (q * jnp.exp(r)).astype(BF)
    last = r[count - 1 : count]
    kf = (k[:count] * jnp.exp(last - r[:count])).astype(BF)
    full = tn_dot(vb[:count], kf)
    half = iota((DK, width), 1)
    state_ref[:DK] = jnp.where(half < DK, full[:DK], full[DK:]).astype(BF)
    state_ref[DK:] = jnp.broadcast_to(jnp.exp(last), (HALO, width)).astype(BF)


def head_kernel(intra_ref, qd_ref, enter_ref, g_ref, halo_ref, gain_ref, out_ref):
    width = intra_ref.shape[1]
    half = iota((DK, width), 1)
    e = enter_ref[...]
    full = jnp.concatenate([jnp.where(half < DK, e, 0.0), jnp.where(half >= DK, e, 0.0)], axis=0)
    rec = intra_ref[...] + nt_dot(qd_ref[...], full.astype(BF))
    ones = head_ones(width)
    sq = rec * rec
    hi = sq.astype(BF)
    lo = (sq - hi.astype(F32)).astype(BF)
    mean = (dot(hi, ones) + dot(lo, ones)) * (1.0 / DK)
    gate = in_order(g_ref[...], halo_ref[:, 3 * width : 4 * width])
    gain = jnp.concatenate([gain_ref[...]] * (width // DK), axis=1)
    out = rec * lax.rsqrt(mean + EPS) * gain * silu(gate)
    out = pltpu.roll(out, out.shape[0] - 2, 0).astype(BF)
    for i in range(out_ref.shape[0]):
        out_ref[i] = out


def stream_kernel(p_ref, heads_ref, *refs):
    n = (len(refs) - 2) // 2
    weights, resid = refs[:n], refs[n : 2 * n]
    normed_ref, own_ref = refs[2 * n :]
    count = own_ref.shape[0]
    p = p_ref[0]
    cw = resid[0].shape[1]
    head = jnp.concatenate(
        [jnp.concatenate([heads_ref[g * n + e] for e in range(n)], axis=1) for g in (p, 1 - p)], axis=0
    )
    parts = []
    total = None
    for d in range(n):
        s = resid[d][...].astype(F32) + dot(head, weights[d][...])
        parts.append(s)
        sq = jnp.sum(s * s, axis=1, keepdims=True)
        total = sq if total is None else total + sq
    own_ref[...] = parts[0][: own_ref.shape[0]]
    scale = lax.rsqrt(total / (n * cw) + EPS)
    for d in range(n):
        g = resid[d][count : count + HALO].astype(F32)
        gain = g[0:1] + g[1:2] + g[2:3]
        normed_ref[:, d * cw : (d + 1) * cw] = (parts[d] * scale * gain).astype(BF)


def mixer_kernel(x_ref, normed_ref, taps_ref, w_hbm, *refs):
    *outs, w, acc, sems = refs
    groups = 2
    n = len(outs) // groups
    count = outs[0].shape[0]
    x = x_ref[0]
    cw = w.shape[0] // n
    up = taps_ref.shape[1]
    half = up // 2
    rows = acc.shape[0] // groups

    def copy(d):
        return pltpu.make_async_copy(
            w_hbm.at[pl.ds(cw * lax.rem(x + d, n), cw), :], w.at[pl.ds(cw * d, cw), :], sems.at[d]
        )

    for d in range(n):
        copy(d).start()
    for d in range(n):
        copy(d).wait()
        part = dot(normed_ref[:, d * cw : (d + 1) * cw], w[d * cw : (d + 1) * cw, :up])
        if d == 0:
            acc[...] = part
        else:
            acc[...] += part
    hidden = []
    for g in range(groups):
        u = acc[g * rows : (g + 1) * rows, :].astype(BF).astype(F32)
        c = (
            taps_ref[0:1] * pltpu.roll(u, 2, 0)
            + taps_ref[8:9] * pltpu.roll(u, 1, 0)
            + taps_ref[16:17] * u
        )[:count]
        gate = pltpu.roll(c, half, 1)[:, :half]
        hidden.append((silu(gate) * c[:, :half]).astype(BF))
    hidden = jnp.concatenate(hidden, axis=0)
    for d in range(n):
        t = nt_dot(hidden, w[d * cw : (d + 1) * cw, up:]).astype(BF)
        for g in range(groups):
            outs[d * groups + g][...] = t[g * count : (g + 1) * count]


def call(kernel, out, *args, scratch=(), specs=None):
    vm = pl.BlockSpec(memory_space=pltpu.VMEM)
    return pl.pallas_call(
        kernel,
        out_shape=out,
        in_specs=specs or [vm] * len(args),
        out_specs=jax.tree.map(lambda _: vm, out),
        scratch_shapes=list(scratch),
    )(*args)


def moved(array, axis, by):
    n = lax.axis_size(axis)
    return lax.ppermute(array, axis, [(i, i + by) for i in range(n) if 0 <= i + by < n])


def from_peers(array):
    n = lax.axis_size("tp")
    return [array] + [
        lax.ppermute(array, "tp", [((i + d) % n, i) for i in range(n)]) for d in range(1, n)
    ]


def from_pair(array):
    return lax.ppermute(array, "grp_1", [(0, 1), (1, 0)])


def entering(packed, beside):
    partner = lax.ppermute(packed, "sp_1", [(0, 1), (1, 0)]).astype(F32)
    own = packed.astype(F32)
    second = lax.axis_index("sp_1") == 1

    def parts(p):
        p = p.astype(F32)
        return p[:DK], p[DK : DK + 1]

    first, later = jnp.where(second, partner, own), jnp.where(second, own, partner)
    s0, d0 = parts(first)
    s1, d1 = parts(later)

    def pack(s, d):
        return jnp.concatenate([s, jnp.broadcast_to(d, (HALO, d.shape[1]))], axis=0).astype(BF)

    chip = pack(d1 * s0 + s1, d0 * d1)
    n = lax.axis_size("sp_0")

    def before(p, shift):
        return parts(moved(p, "sp_0", shift))

    (state, decay), (s, d) = before(chip, 1), before(chip, 2)
    state, decay = state + decay * s, decay * d
    shift = 2
    while shift < n:
        s, d = before(pack(state, decay), shift)
        state, decay = state + decay * s, decay * d
        if shift == 2:
            state, *beside[:] = lax.optimization_barrier((state, *beside))
        shift *= 2
    return jnp.where(second, d0 * state + s0, state)


def on_device(
    residual_in,
    query_pre,
    forget_pre,
    value_pre,
    gate_pre,
    floor_gap,
    head_gain,
    out_weight,
    norm_gain,
    value_weight,
    gate_weight,
    value_taps,
    gate_taps,
    down_weight,
):
    count, cols = residual_in.shape
    width = query_pre.shape[1]
    rows = count + HALO
    n = lax.axis_size("tp")
    x = lax.axis_index("tp").astype(jnp.int32).reshape(1)
    p = lax.axis_index("grp_1").astype(jnp.int32).reshape(1)
    up = value_weight.shape[1]
    vm = pl.BlockSpec(memory_space=pltpu.VMEM)
    sm = pl.BlockSpec(memory_space=pltpu.SMEM)
    hbm = pl.BlockSpec(memory_space=pl.ANY)
    sd = jax.ShapeDtypeStruct
    share = call(
        share_kernel,
        sd((value_weight.shape[0], up + up // 2), BF),
        p,
        value_weight,
        gate_weight,
        down_weight.T,
        specs=[sm] + [vm] * 3,
    )
    share, p = lax.optimization_barrier((share, p))
    gathered = lax.all_gather(share, SP, axis=0, tiled=True)
    tails, taps = call(
        prep_kernel,
        (sd((HALO, 4 * width + cols), BF), sd((8 * value_taps.shape[0], up), F32)),
        p,
        value_taps,
        gate_taps,
        query_pre,
        forget_pre,
        value_pre,
        gate_pre,
        residual_in,
        specs=[sm] + [vm] * 7,
    )
    weights = from_peers(out_weight)
    halo = moved(tails, SP, 1)
    intra, qd, packed, resid = call(
        local_kernel,
        (sd((rows, width), F32), sd((rows, width), BF), sd((DK + HALO, width), BF), sd((rows, cols), BF)),
        query_pre,
        forget_pre,
        value_pre,
        halo,
        floor_gap.reshape(1, width),
        residual_in,
        norm_gain.reshape(1, cols),
    )
    beside = [from_pair(resid), *weights[1:]]
    enter = entering(packed, beside)
    pair, *weights[1:] = beside
    resids = from_peers(jnp.concatenate([resid, pair], axis=0))
    enter, *resids[1:] = lax.optimization_barrier((enter, *resids[1:]))
    head = call(
        head_kernel,
        sd((2 * n, rows, width), BF),
        intra,
        qd,
        enter,
        gate_pre,
        halo,
        head_gain.reshape(1, DK),
    )
    heads = lax.all_to_all(head, PAIR, 0, 0, tiled=True)
    normed, own = call(
        stream_kernel,
        (sd((2 * rows, n * cols), BF), sd((count, cols), F32)),
        p,
        heads,
        *weights,
        *resids,
        specs=[sm] + [vm] * (2 * n + 1),
    )
    terms = call(
        mixer_kernel,
        (sd((count, cols), BF),) * (2 * n),
        x,
        normed,
        taps,
        gathered,
        specs=[sm, vm, vm, hbm],
        scratch=(
            pltpu.VMEM(gathered.shape, BF),
            pltpu.VMEM((2 * rows, up), F32),
            pltpu.SemaphoreType.DMA((n,)),
        ),
    )
    total = own + terms[0].astype(F32)
    far = n // 2
    near = [d for d in range(n - 1, 0, -1) if d != far]
    order = [(far, 1)] + [(d, 0) for d in near] + [(far, 0), (0, 1)] + [(d, 1) for d in near]
    for d, g in order:
        perm = [(j * n + i, (j ^ g) * n + (i + d) % n) for j in range(2) for i in range(n)]
        total = total + lax.ppermute(terms[2 * d + g], PAIR, perm).astype(F32)
    return total.astype(BF)


def solution(mesh):
    groups, seq, tp = (mesh.shape[a] for a in ("grp", "sp", "tp"))
    finer = Mesh(
        mesh.devices.reshape(groups // 2, 2, seq // 2, 2, tp), (*GRP, *SP, "tp")
    )
    rows = P((*GRP, *SP), "tp")
    placed = (
        *[rows] * 5,
        P("tp"),
        P(),
        P(None, "tp"),
        P("tp"),
        P(SP, "tp"),
        P(SP, "tp"),
        P(None, "tp"),
        P(None, "tp"),
        P("tp", SP),
    )
    return jax.shard_map(on_device, mesh=finer, in_specs=placed, out_specs=rows, check_vma=False)
```

```python
import jax
import jax.numpy as jnp
from jax import lax
from jax.experimental import pallas as pl
from jax.experimental.pallas import tpu as pltpu
from jax.sharding import Mesh
from jax.sharding import PartitionSpec as P

BF = jnp.bfloat16
F32 = jnp.float32
EPS = 1e-06
DK = 64
SP = ("sp_0", "sp_1")
GRP = ("grp_0", "grp_1")
PAIR = ("grp_1", "tp")
HALO = 16
CH = 16


def silu(v):
    return v / (1.0 + jnp.exp(-v))


def nt_dot(a, b):
    return lax.dot_general(a, b, (((1,), (1,)), ((), ())), preferred_element_type=F32)


def tn_dot(a, b):
    return lax.dot_general(a, b, (((0,), (0,)), ((), ())), preferred_element_type=F32)


def dot(a, b):
    return jnp.dot(a, b, preferred_element_type=F32)


def iota(shape, dim):
    return lax.broadcasted_iota(jnp.int32, shape, dim)


def in_order(rows, halo):
    count = rows.shape[0]
    both = jnp.concatenate([rows.astype(F32), halo.astype(F32)], axis=0)
    row = iota(both.shape, 0)
    both = jnp.where((row >= count) & (row < count + HALO - 2), 0.0, both)
    return pltpu.roll(both, 2, 0)


def head_ones(width):
    a = iota((width, width), 0) // DK
    b = iota((width, width), 1) // DK
    return jnp.where(a == b, 1.0, 0.0).astype(BF)


def halves(first, v, g):
    v, g = v.astype(F32), g.astype(F32)
    half = v.shape[1] // 2
    lane = iota(v.shape, 1)
    vs = jnp.where(first, v, pltpu.roll(v, half, 1))
    gs = jnp.where(first, pltpu.roll(g, half, 1), g)
    return jnp.where(lane < half, vs, gs)


def share_kernel(p_ref, value_ref, gate_ref, down_ref, share_ref):
    up = value_ref.shape[1]
    half = up // 2
    lane = iota(value_ref.shape, 1)

    def rolled(ref):
        return pltpu.roll(ref[...].astype(F32), half, 1).astype(BF)

    @pl.when(p_ref[0] == 0)
    def _():
        share_ref[:, :up] = jnp.where(lane < half, value_ref[...], rolled(gate_ref))
        share_ref[:, up:] = down_ref[:, :half]

    @pl.when(p_ref[0] != 0)
    def _():
        share_ref[:, :up] = jnp.where(lane < half, rolled(value_ref), gate_ref[...])
        share_ref[:, up:] = rolled(down_ref)[:, :half]


def prep_kernel(p_ref, vt_ref, gt_ref, *refs):
    *parts, tails_ref, taps_ref = refs
    first = p_ref[0] == 0
    up = vt_ref.shape[1]
    for i in range(vt_ref.shape[0]):
        v = jnp.broadcast_to(vt_ref[i : i + 1], (8, up))
        g = jnp.broadcast_to(gt_ref[i : i + 1], (8, up))
        taps_ref[8 * i : 8 * i + 8] = halves(first, v, g)
    at = 0
    for part in parts:
        count, width = part.shape
        tails_ref[:, at : at + width] = part[count - HALO :, :]
        at += width


def local_kernel(q_ref, f_ref, v_ref, halo_ref, gap_ref, res_ref, gain_ref, intra_ref, qd_ref, state_ref, ext_ref):
    count, width = q_ref.shape
    ext_ref[:count] = res_ref[...]
    gain = gain_ref[...]
    g0 = gain.astype(BF).astype(F32)
    g1 = (gain - g0).astype(BF).astype(F32)
    g2 = gain - g0 - g1
    tail = halo_ref[:, 4 * width :].astype(F32)
    place = iota(tail.shape, 0)
    tail = jnp.where(place < HALO - 2, 0.0, tail)
    for i, g in enumerate((g0, g1, g2)):
        tail = jnp.where(place == i, g, tail)
    ext_ref[count:] = tail.astype(BF)
    q = silu(in_order(q_ref[...], halo_ref[:, 0:width]))
    f = in_order(f_ref[...], halo_ref[:, width : 2 * width])
    v = in_order(v_ref[...], halo_ref[:, 2 * width : 3 * width])
    rows = q.shape[0]
    k = gap_ref[...] / (1.0 + jnp.exp(f))
    a = 1.0 - k
    la = jnp.log(a)
    row = iota(q.shape, 0)
    lane = iota((CH, width), 1)
    r = la
    step = 1
    while step < rows:
        r = r + jnp.where(row >= step, pltpu.roll(r, step, 0), 0.0)
        step *= 2
    ones = head_ones(width)
    inside = row % CH
    decay = jnp.ones_like(q)
    out = jnp.zeros_like(q)
    for j in range(CH):
        if j:
            decay = decay * (pltpu.roll(a, j - 1, 0) if j > 1 else a)
        kj = pltpu.roll(k, j, 0) if j else k
        vj = pltpu.roll(v, j, 0) if j else v
        term = jnp.where(inside >= j, q * decay * kj, 0.0)
        out = out + dot(term.astype(BF), ones) * vj
    pieces = [out[:CH]]
    vb = v.astype(BF)
    for i in range(1, rows // CH):
        lo = i * CH
        start = r[lo - 1 : lo]
        qi = q[lo : lo + CH] * jnp.exp(r[lo : lo + CH] - start)
        qi = jnp.concatenate([jnp.where(lane < DK, qi, 0.0), jnp.where(lane >= DK, qi, 0.0)], axis=0)
        ki = k[:lo] * jnp.exp(start - r[:lo])
        both = dot(nt_dot(qi.astype(BF), ki.astype(BF)).astype(BF), vb[:lo])
        pieces.append(out[lo : lo + CH] + jnp.where(lane < DK, both[:CH], both[CH:]))
    intra_ref[...] = jnp.concatenate(pieces, axis=0)
    qd_ref[...] = (q * jnp.exp(r)).astype(BF)
    last = r[count - 1 : count]
    kf = (k[:count] * jnp.exp(last - r[:count])).astype(BF)
    full = tn_dot(vb[:count], kf)
    half = iota((DK, width), 1)
    state_ref[:DK] = jnp.where(half < DK, full[:DK], full[DK:]).astype(BF)
    state_ref[DK:] = jnp.broadcast_to(jnp.exp(last), (HALO, width)).astype(BF)


def head_kernel(intra_ref, qd_ref, enter_ref, g_ref, halo_ref, gain_ref, out_ref):
    width = intra_ref.shape[1]
    half = iota((DK, width), 1)
    e = enter_ref[...]
    full = jnp.concatenate([jnp.where(half < DK, e, 0.0), jnp.where(half >= DK, e, 0.0)], axis=0)
    rec = intra_ref[...] + nt_dot(qd_ref[...], full.astype(BF))
    ones = head_ones(width)
    sq = rec * rec
    hi = sq.astype(BF)
    lo = (sq - hi.astype(F32)).astype(BF)
    mean = (dot(hi, ones) + dot(lo, ones)) * (1.0 / DK)
    gate = in_order(g_ref[...], halo_ref[:, 3 * width : 4 * width])
    gain = jnp.concatenate([gain_ref[...]] * (width // DK), axis=1)
    out = rec * lax.rsqrt(mean + EPS) * gain * silu(gate)
    out = pltpu.roll(out, out.shape[0] - 2, 0).astype(BF)
    for i in range(out_ref.shape[0]):
        out_ref[i] = out


def stream_kernel(p_ref, heads_ref, *refs):
    n = (len(refs) - 2) // 2
    weights, resid = refs[:n], refs[n : 2 * n]
    normed_ref, own_ref = refs[2 * n :]
    count = own_ref.shape[0]
    p = p_ref[0]
    cw = resid[0].shape[1]
    head = jnp.concatenate(
        [jnp.concatenate([heads_ref[g * n + e] for e in range(n)], axis=1) for g in (p, 1 - p)], axis=0
    )
    parts = []
    total = None
    for d in range(n):
        s = resid[d][...].astype(F32) + dot(head, weights[d][...])
        parts.append(s)
        sq = jnp.sum(s * s, axis=1, keepdims=True)
        total = sq if total is None else total + sq
    own_ref[...] = parts[0][: own_ref.shape[0]]
    scale = lax.rsqrt(total / (n * cw) + EPS)
    for d in range(n):
        g = resid[d][count : count + HALO].astype(F32)
        gain = g[0:1] + g[1:2] + g[2:3]
        normed_ref[:, d * cw : (d + 1) * cw] = (parts[d] * scale * gain).astype(BF)


def mixer_kernel(x_ref, normed_ref, taps_ref, w_hbm, *refs):
    *outs, w, acc, sems = refs
    groups = 2
    n = len(outs) // groups
    count = outs[0].shape[0]
    x = x_ref[0]
    cw = w.shape[0] // n
    up = taps_ref.shape[1]
    half = up // 2
    rows = acc.shape[0] // groups

    def copy(d):
        return pltpu.make_async_copy(
            w_hbm.at[pl.ds(cw * lax.rem(x + d, n), cw), :], w.at[pl.ds(cw * d, cw), :], sems.at[d]
        )

    for d in range(n):
        copy(d).start()
    for d in range(n):
        copy(d).wait()
        part = dot(normed_ref[:, d * cw : (d + 1) * cw], w[d * cw : (d + 1) * cw, :up])
        if d == 0:
            acc[...] = part
        else:
            acc[...] += part
    hidden = []
    for g in range(groups):
        u = acc[g * rows : (g + 1) * rows, :].astype(BF).astype(F32)
        c = (
            taps_ref[0:1] * pltpu.roll(u, 2, 0)
            + taps_ref[8:9] * pltpu.roll(u, 1, 0)
            + taps_ref[16:17] * u
        )[:count]
        gate = pltpu.roll(c, half, 1)[:, :half]
        hidden.append((silu(gate) * c[:, :half]).astype(BF))
    hidden = jnp.concatenate(hidden, axis=0)
    for d in range(n):
        t = nt_dot(hidden, w[d * cw : (d + 1) * cw, up:]).astype(BF)
        for g in range(groups):
            outs[d * groups + g][...] = t[g * count : (g + 1) * count]


def call(kernel, out, *args, scratch=(), specs=None):
    vm = pl.BlockSpec(memory_space=pltpu.VMEM)
    return pl.pallas_call(
        kernel,
        out_shape=out,
        in_specs=specs or [vm] * len(args),
        out_specs=jax.tree.map(lambda _: vm, out),
        scratch_shapes=list(scratch),
    )(*args)


def moved(array, axis, by):
    n = lax.axis_size(axis)
    return lax.ppermute(array, axis, [(i, i + by) for i in range(n) if 0 <= i + by < n])


def from_peers(array):
    n = lax.axis_size("tp")
    return [array] + [
        lax.ppermute(array, "tp", [((i + d) % n, i) for i in range(n)]) for d in range(1, n)
    ]


def from_pair(array):
    return lax.ppermute(array, "grp_1", [(0, 1), (1, 0)])


def entering(packed, beside):
    partner = lax.ppermute(packed, "sp_1", [(0, 1), (1, 0)]).astype(F32)
    own = packed.astype(F32)
    second = lax.axis_index("sp_1") == 1

    def parts(p):
        p = p.astype(F32)
        return p[:DK], p[DK : DK + 1]

    first, later = jnp.where(second, partner, own), jnp.where(second, own, partner)
    s0, d0 = parts(first)
    s1, d1 = parts(later)

    def pack(s, d):
        return jnp.concatenate([s, jnp.broadcast_to(d, (HALO, d.shape[1]))], axis=0).astype(BF)

    chip = pack(d1 * s0 + s1, d0 * d1)
    n = lax.axis_size("sp_0")

    def before(p, shift):
        return parts(moved(p, "sp_0", shift))

    (state, decay), (s, d) = before(chip, 1), before(chip, 2)
    state, decay = state + decay * s, decay * d
    shift = 2
    while shift < n:
        s, d = before(pack(state, decay), shift)
        state, decay = state + decay * s, decay * d
        if shift == 2:
            state, *beside[:] = lax.optimization_barrier((state, *beside))
        shift *= 2
    return jnp.where(second, d0 * state + s0, state)


def on_device(
    residual_in,
    query_pre,
    forget_pre,
    value_pre,
    gate_pre,
    floor_gap,
    head_gain,
    out_weight,
    norm_gain,
    value_weight,
    gate_weight,
    value_taps,
    gate_taps,
    down_weight,
):
    count, cols = residual_in.shape
    width = query_pre.shape[1]
    rows = count + HALO
    n = lax.axis_size("tp")
    x = lax.axis_index("tp").astype(jnp.int32).reshape(1)
    p = lax.axis_index("grp_1").astype(jnp.int32).reshape(1)
    up = value_weight.shape[1]
    vm = pl.BlockSpec(memory_space=pltpu.VMEM)
    sm = pl.BlockSpec(memory_space=pltpu.SMEM)
    hbm = pl.BlockSpec(memory_space=pl.ANY)
    sd = jax.ShapeDtypeStruct
    share = call(
        share_kernel,
        sd((value_weight.shape[0], up + up // 2), BF),
        p,
        value_weight,
        gate_weight,
        down_weight.T,
        specs=[sm] + [vm] * 3,
    )
    share, p = lax.optimization_barrier((share, p))
    gathered = lax.all_gather(share, SP, axis=0, tiled=True)
    tails, taps = call(
        prep_kernel,
        (sd((HALO, 4 * width + cols), BF), sd((8 * value_taps.shape[0], up), F32)),
        p,
        value_taps,
        gate_taps,
        query_pre,
        forget_pre,
        value_pre,
        gate_pre,
        residual_in,
        specs=[sm] + [vm] * 7,
    )
    weights = from_peers(out_weight)
    halo = moved(tails, SP, 1)
    intra, qd, packed, resid = call(
        local_kernel,
        (sd((rows, width), F32), sd((rows, width), BF), sd((DK + HALO, width), BF), sd((rows, cols), BF)),
        query_pre,
        forget_pre,
        value_pre,
        halo,
        floor_gap.reshape(1, width),
        residual_in,
        norm_gain.reshape(1, cols),
    )
    beside = [from_pair(resid)]
    enter = entering(packed, beside)
    (pair,) = beside
    resids = from_peers(jnp.concatenate([resid, pair], axis=0))
    enter, *resids[1:] = lax.optimization_barrier((enter, *resids[1:]))
    head = call(
        head_kernel,
        sd((2 * n, rows, width), BF),
        intra,
        qd,
        enter,
        gate_pre,
        halo,
        head_gain.reshape(1, DK),
    )
    heads = lax.all_to_all(head, PAIR, 0, 0, tiled=True)
    normed, own = call(
        stream_kernel,
        (sd((2 * rows, n * cols), BF), sd((count, cols), F32)),
        p,
        heads,
        *weights,
        *resids,
        specs=[sm] + [vm] * (2 * n + 1),
    )
    terms = call(
        mixer_kernel,
        (sd((count, cols), BF),) * (2 * n),
        x,
        normed,
        taps,
        gathered,
        specs=[sm, vm, vm, hbm],
        scratch=(
            pltpu.VMEM(gathered.shape, BF),
            pltpu.VMEM((2 * rows, up), F32),
            pltpu.SemaphoreType.DMA((n,)),
        ),
    )
    total = own + terms[0].astype(F32)
    far = n // 2
    near = [d for d in range(n - 1, 0, -1) if d != far]
    order = [(far, 1), (0, 1)] + [(d, g) for d in near for g in (0, 1)] + [(far, 0)]
    for k, (d, g) in enumerate(order):
        if k == n:
            total = lax.optimization_barrier(total)
        perm = [(j * n + i, (j ^ g) * n + (i + d) % n) for j in range(2) for i in range(n)]
        total = total + lax.ppermute(terms[2 * d + g], PAIR, perm).astype(F32)
    return total.astype(BF)


def solution(mesh):
    groups, seq, tp = (mesh.shape[a] for a in ("grp", "sp", "tp"))
    finer = Mesh(
        mesh.devices.reshape(groups // 2, 2, seq // 2, 2, tp), (*GRP, *SP, "tp")
    )
    rows = P((*GRP, *SP), "tp")
    placed = (
        *[rows] * 5,
        P("tp"),
        P(),
        P(None, "tp"),
        P("tp"),
        P(SP, "tp"),
        P(SP, "tp"),
        P(None, "tp"),
        P(None, "tp"),
        P("tp", SP),
    )

    return jax.shard_map(on_device, mesh=finer, in_specs=placed, out_specs=rows, check_vma=False)
```

```python
import jax
import jax.numpy as jnp
from jax import lax
from jax.experimental import pallas as pl
from jax.experimental.pallas import tpu as pltpu
from jax.sharding import Mesh
from jax.sharding import PartitionSpec as P

BF = jnp.bfloat16
F32 = jnp.float32
EPS = 1e-06
DK = 64
SP = ("sp_0", "sp_1")
GRP = ("grp_0", "grp_1")
PAIR = ("grp_1", "tp")
HALO = 16
CH = 16


def silu(v):
    return v / (1.0 + jnp.exp(-v))


def nt_dot(a, b):
    return lax.dot_general(a, b, (((1,), (1,)), ((), ())), preferred_element_type=F32)


def tn_dot(a, b):
    return lax.dot_general(a, b, (((0,), (0,)), ((), ())), preferred_element_type=F32)


def dot(a, b):
    return jnp.dot(a, b, preferred_element_type=F32)


def iota(shape, dim):
    return lax.broadcasted_iota(jnp.int32, shape, dim)


def in_order(rows, halo):
    count = rows.shape[0]
    both = jnp.concatenate([rows.astype(F32), halo.astype(F32)], axis=0)
    row = iota(both.shape, 0)
    both = jnp.where((row >= count) & (row < count + HALO - 2), 0.0, both)
    return pltpu.roll(both, 2, 0)


def head_ones(width):
    a = iota((width, width), 0) // DK
    b = iota((width, width), 1) // DK
    return jnp.where(a == b, 1.0, 0.0).astype(BF)


def halves(first, v, g):
    v, g = v.astype(F32), g.astype(F32)
    half = v.shape[1] // 2
    lane = iota(v.shape, 1)
    vs = jnp.where(first, v, pltpu.roll(v, half, 1))
    gs = jnp.where(first, pltpu.roll(g, half, 1), g)
    return jnp.where(lane < half, vs, gs)


def share_kernel(p_ref, value_ref, gate_ref, down_ref, share_ref):
    up = value_ref.shape[1]
    half = up // 2
    lane = iota(value_ref.shape, 1)

    def rolled(ref):
        return pltpu.roll(ref[...].astype(F32), half, 1).astype(BF)

    @pl.when(p_ref[0] == 0)
    def _():
        share_ref[:, :up] = jnp.where(lane < half, value_ref[...], rolled(gate_ref))
        share_ref[:, up:] = down_ref[:, :half]

    @pl.when(p_ref[0] != 0)
    def _():
        share_ref[:, :up] = jnp.where(lane < half, rolled(value_ref), gate_ref[...])
        share_ref[:, up:] = rolled(down_ref)[:, :half]


def prep_kernel(p_ref, vt_ref, gt_ref, *refs):
    *parts, tails_ref, taps_ref = refs
    first = p_ref[0] == 0
    up = vt_ref.shape[1]
    for i in range(vt_ref.shape[0]):
        v = jnp.broadcast_to(vt_ref[i : i + 1], (8, up))
        g = jnp.broadcast_to(gt_ref[i : i + 1], (8, up))
        taps_ref[8 * i : 8 * i + 8] = halves(first, v, g)
    at = 0
    for part in parts:
        count, width = part.shape
        tails_ref[:, at : at + width] = part[count - HALO :, :]
        at += width


def local_kernel(q_ref, f_ref, v_ref, halo_ref, gap_ref, res_ref, gain_ref, intra_ref, qd_ref, state_ref, ext_ref):
    count, width = q_ref.shape
    ext_ref[:count] = res_ref[...]
    gain = gain_ref[...]
    g0 = gain.astype(BF).astype(F32)
    g1 = (gain - g0).astype(BF).astype(F32)
    g2 = gain - g0 - g1
    tail = halo_ref[:, 4 * width :].astype(F32)
    place = iota(tail.shape, 0)
    tail = jnp.where(place < HALO - 2, 0.0, tail)
    for i, g in enumerate((g0, g1, g2)):
        tail = jnp.where(place == i, g, tail)
    ext_ref[count:] = tail.astype(BF)
    q = silu(in_order(q_ref[...], halo_ref[:, 0:width]))
    f = in_order(f_ref[...], halo_ref[:, width : 2 * width])
    v = in_order(v_ref[...], halo_ref[:, 2 * width : 3 * width])
    rows = q.shape[0]
    k = gap_ref[...] / (1.0 + jnp.exp(f))
    a = 1.0 - k
    la = jnp.log(a)
    row = iota(q.shape, 0)
    lane = iota((CH, width), 1)
    r = la
    step = 1
    while step < rows:
        r = r + jnp.where(row >= step, pltpu.roll(r, step, 0), 0.0)
        step *= 2
    ones = head_ones(width)
    inside = row % CH
    decay = jnp.ones_like(q)
    out = jnp.zeros_like(q)
    for j in range(CH):
        if j:
            decay = decay * (pltpu.roll(a, j - 1, 0) if j > 1 else a)
        kj = pltpu.roll(k, j, 0) if j else k
        vj = pltpu.roll(v, j, 0) if j else v
        term = jnp.where(inside >= j, q * decay * kj, 0.0)
        out = out + dot(term.astype(BF), ones) * vj
    pieces = [out[:CH]]
    vb = v.astype(BF)
    for i in range(1, rows // CH):
        lo = i * CH
        start = r[lo - 1 : lo]
        qi = q[lo : lo + CH] * jnp.exp(r[lo : lo + CH] - start)
        qi = jnp.concatenate([jnp.where(lane < DK, qi, 0.0), jnp.where(lane >= DK, qi, 0.0)], axis=0)
        ki = k[:lo] * jnp.exp(start - r[:lo])
        both = dot(nt_dot(qi.astype(BF), ki.astype(BF)).astype(BF), vb[:lo])
        pieces.append(out[lo : lo + CH] + jnp.where(lane < DK, both[:CH], both[CH:]))
    intra_ref[...] = jnp.concatenate(pieces, axis=0)
    qd_ref[...] = (q * jnp.exp(r)).astype(BF)
    last = r[count - 1 : count]
    kf = (k[:count] * jnp.exp(last - r[:count])).astype(BF)
    full = tn_dot(vb[:count], kf)
    half = iota((DK, width), 1)
    state_ref[:DK] = jnp.where(half < DK, full[:DK], full[DK:]).astype(BF)
    state_ref[DK:] = jnp.broadcast_to(jnp.exp(last), (HALO, width)).astype(BF)


def head_kernel(intra_ref, qd_ref, enter_ref, g_ref, halo_ref, gain_ref, out_ref):
    width = intra_ref.shape[1]
    half = iota((DK, width), 1)
    e = enter_ref[...]
    full = jnp.concatenate([jnp.where(half < DK, e, 0.0), jnp.where(half >= DK, e, 0.0)], axis=0)
    rec = intra_ref[...] + nt_dot(qd_ref[...], full.astype(BF))
    ones = head_ones(width)
    sq = rec * rec
    hi = sq.astype(BF)
    lo = (sq - hi.astype(F32)).astype(BF)
    mean = (dot(hi, ones) + dot(lo, ones)) * (1.0 / DK)
    gate = in_order(g_ref[...], halo_ref[:, 3 * width : 4 * width])
    gain = jnp.concatenate([gain_ref[...]] * (width // DK), axis=1)
    out = rec * lax.rsqrt(mean + EPS) * gain * silu(gate)
    out = pltpu.roll(out, out.shape[0] - 2, 0).astype(BF)
    for i in range(out_ref.shape[0]):
        out_ref[i] = out


def stream_kernel(p_ref, heads_ref, *refs):
    n = (len(refs) - 2) // 2
    weights, resid = refs[:n], refs[n : 2 * n]
    normed_ref, own_ref = refs[2 * n :]
    count = own_ref.shape[0]
    p = p_ref[0]
    cw = resid[0].shape[1]
    head = jnp.concatenate(
        [jnp.concatenate([heads_ref[g * n + e] for e in range(n)], axis=1) for g in (p, 1 - p)], axis=0
    )
    parts = []
    total = None
    for d in range(n):
        s = resid[d][...].astype(F32) + dot(head, weights[d][...])
        parts.append(s)
        sq = jnp.sum(s * s, axis=1, keepdims=True)
        total = sq if total is None else total + sq
    own_ref[...] = parts[0][: own_ref.shape[0]]
    scale = lax.rsqrt(total / (n * cw) + EPS)
    for d in range(n):
        g = resid[d][count : count + HALO].astype(F32)
        gain = g[0:1] + g[1:2] + g[2:3]
        normed_ref[d] = (parts[d] * scale * gain).astype(BF)


def mixer_kernel(x_ref, normed_hbm, taps_ref, w_hbm, *refs):
    *outs, w, normed, acc, out, wsems, nsems, osems = refs
    groups = 2
    n = len(outs) // groups
    count = outs[0].shape[0]
    x = x_ref[0]
    cw = w.shape[0] // n
    up = taps_ref.shape[1]
    half = up // 2
    rows = acc.shape[0] // groups
    plan = [(d, 0, cw) for d in range(n - 1)] + [(n - 1, 0, cw // 2), (n - 1, cw // 2, cw // 2)]
    blocks = [pltpu.make_async_copy(normed_hbm.at[d], normed.at[d], nsems.at[d]) for d in range(n)]
    chunks = [
        pltpu.make_async_copy(
            w_hbm.at[pl.ds(cw * lax.rem(x + d, n) + at, size), :],
            w.at[pl.ds(cw * d + at, size), :],
            wsems.at[i],
        )
        for i, (d, at, size) in enumerate(plan)
    ]
    for (d, at, _), chunk in zip(plan, chunks):
        if at == 0:
            blocks[d].start()
        chunk.start()
    for (d, at, size), chunk in zip(plan, chunks):
        if at == 0:
            blocks[d].wait()
        chunk.wait()
        to = d * cw + at
        part = dot(normed[d][:, at : at + size], w[to : to + size, :up])
        if to == 0:
            acc[...] = part
        else:
            acc[...] += part
    hidden = []
    for g in range(groups):
        u = acc[g * rows : (g + 1) * rows, :].astype(BF).astype(F32)
        c = (
            taps_ref[0:1] * pltpu.roll(u, 2, 0)
            + taps_ref[8:9] * pltpu.roll(u, 1, 0)
            + taps_ref[16:17] * u
        )[:count]
        gate = pltpu.roll(c, half, 1)[:, :half]
        hidden.append((silu(gate) * c[:, :half]).astype(BF))
    hidden = jnp.concatenate(hidden, axis=0)
    writes = []
    for d in range(n):
        t = nt_dot(hidden, w[d * cw : (d + 1) * cw, up:]).astype(BF)
        for g in range(groups):
            i = d * groups + g
            out[i] = t[g * count : (g + 1) * count]
            writes.append(pltpu.make_async_copy(out.at[i], outs[i], osems.at[i]))
            writes[-1].start()
    for write in writes:
        write.wait()


def call(kernel, out, *args, scratch=(), specs=None, results=None):
    vm = pl.BlockSpec(memory_space=pltpu.VMEM)
    return pl.pallas_call(
        kernel,
        out_shape=out,
        in_specs=specs or [vm] * len(args),
        out_specs=jax.tree.map(lambda _: results or vm, out),
        scratch_shapes=list(scratch),
    )(*args)


def moved(array, axis, by):
    n = lax.axis_size(axis)
    return lax.ppermute(array, axis, [(i, i + by) for i in range(n) if 0 <= i + by < n])


def from_peers(array):
    n = lax.axis_size("tp")
    return [array] + [
        lax.ppermute(array, "tp", [((i + d) % n, i) for i in range(n)]) for d in range(1, n)
    ]


def from_pair(array):
    return lax.ppermute(array, "grp_1", [(0, 1), (1, 0)])


def entering(packed, beside):
    partner = lax.ppermute(packed, "sp_1", [(0, 1), (1, 0)]).astype(F32)
    own = packed.astype(F32)
    second = lax.axis_index("sp_1") == 1

    def parts(p):
        p = p.astype(F32)
        return p[:DK], p[DK : DK + 1]

    first, later = jnp.where(second, partner, own), jnp.where(second, own, partner)
    s0, d0 = parts(first)
    s1, d1 = parts(later)

    def pack(s, d):
        return jnp.concatenate([s, jnp.broadcast_to(d, (HALO, d.shape[1]))], axis=0).astype(BF)

    chip = pack(d1 * s0 + s1, d0 * d1)
    n = lax.axis_size("sp_0")

    def before(p, shift):
        return parts(moved(p, "sp_0", shift))

    (state, decay), (s, d) = before(chip, 1), before(chip, 2)
    state, decay = state + decay * s, decay * d
    shift = 2
    while shift < n:
        s, d = before(pack(state, decay), shift)
        state, decay = state + decay * s, decay * d
        if shift == 2:
            state, *beside[:] = lax.optimization_barrier((state, *beside))
        shift *= 2
    return jnp.where(second, d0 * state + s0, state)


def on_device(
    residual_in,
    query_pre,
    forget_pre,
    value_pre,
    gate_pre,
    floor_gap,
    head_gain,
    out_weight,
    norm_gain,
    value_weight,
    gate_weight,
    value_taps,
    gate_taps,
    down_weight,
):
    count, cols = residual_in.shape
    width = query_pre.shape[1]
    rows = count + HALO
    n = lax.axis_size("tp")
    x = lax.axis_index("tp").astype(jnp.int32).reshape(1)
    p = lax.axis_index("grp_1").astype(jnp.int32).reshape(1)
    up = value_weight.shape[1]
    vm = pl.BlockSpec(memory_space=pltpu.VMEM)
    sm = pl.BlockSpec(memory_space=pltpu.SMEM)
    hbm = pl.BlockSpec(memory_space=pl.ANY)
    sd = jax.ShapeDtypeStruct
    share = call(
        share_kernel,
        sd((value_weight.shape[0], up + up // 2), BF),
        p,
        value_weight,
        gate_weight,
        down_weight.T,
        specs=[sm] + [vm] * 3,
    )
    share, p = lax.optimization_barrier((share, p))
    gathered = lax.all_gather(share, SP, axis=0, tiled=True)
    tails, taps = call(
        prep_kernel,
        (sd((HALO, 4 * width + cols), BF), sd((8 * value_taps.shape[0], up), F32)),
        p,
        value_taps,
        gate_taps,
        query_pre,
        forget_pre,
        value_pre,
        gate_pre,
        residual_in,
        specs=[sm] + [vm] * 7,
    )
    weights = from_peers(out_weight)
    halo = moved(tails, SP, 1)
    intra, qd, packed, resid = call(
        local_kernel,
        (sd((rows, width), F32), sd((rows, width), BF), sd((DK + HALO, width), BF), sd((rows, cols), BF)),
        query_pre,
        forget_pre,
        value_pre,
        halo,
        floor_gap.reshape(1, width),
        residual_in,
        norm_gain.reshape(1, cols),
    )
    beside = [from_pair(resid)]
    enter = entering(packed, beside)
    (pair,) = beside
    resids = from_peers(jnp.concatenate([resid, pair], axis=0))
    enter, *resids[1:] = lax.optimization_barrier((enter, *resids[1:]))
    head = call(
        head_kernel,
        sd((2 * n, rows, width), BF),
        intra,
        qd,
        enter,
        gate_pre,
        halo,
        head_gain.reshape(1, DK),
    )
    heads = lax.all_to_all(head, PAIR, 0, 0, tiled=True)
    normed, own = call(
        stream_kernel,
        (sd((n, 2 * rows, cols), BF), sd((count, cols), F32)),
        p,
        heads,
        *weights,
        *resids,
        specs=[sm] + [vm] * (2 * n + 1),
    )
    terms = call(
        mixer_kernel,
        (sd((count, cols), BF),) * (2 * n),
        x,
        normed,
        taps,
        gathered,
        specs=[sm, hbm, vm, hbm],
        results=hbm,
        scratch=(
            pltpu.VMEM(gathered.shape, BF),
            pltpu.VMEM((n, 2 * rows, cols), BF),
            pltpu.VMEM((2 * rows, up), F32),
            pltpu.VMEM((2 * n, count, cols), BF),
            pltpu.SemaphoreType.DMA((n + 1,)),
            pltpu.SemaphoreType.DMA((n,)),
            pltpu.SemaphoreType.DMA((2 * n,)),
        ),
    )
    total = own + terms[0].astype(F32)
    far = n // 2
    near = [d for d in range(n - 1, 0, -1) if d != far]
    order = [(far, 1), (far, 0)] + [(d, 0) for d in near] + [(0, 1)] + [(d, 1) for d in near]
    for k, (d, g) in enumerate(order):
        if k == n:
            total = lax.optimization_barrier(total)
        perm = [(j * n + i, (j ^ g) * n + (i + d) % n) for j in range(2) for i in range(n)]
        total = total + lax.ppermute(terms[2 * d + g], PAIR, perm).astype(F32)
    return total.astype(BF)


def solution(mesh):
    groups, seq, tp = (mesh.shape[a] for a in ("grp", "sp", "tp"))
    finer = Mesh(
        mesh.devices.reshape(groups // 2, 2, seq // 2, 2, tp), (*GRP, *SP, "tp")
    )
    rows = P((*GRP, *SP), "tp")
    placed = (
        *[rows] * 5,
        P("tp"),
        P(),
        P(None, "tp"),
        P("tp"),
        P(SP, "tp"),
        P(SP, "tp"),
        P(None, "tp"),
        P(None, "tp"),
        P("tp", SP),
    )

    return jax.shard_map(on_device, mesh=finer, in_specs=placed, out_specs=rows, check_vma=False)
```
